32 devices in a mesh: sp: 8 (over z, y), dp: 4 (over x, core).
Axes of the slice: x: 2, y: 2, z: 4, core: 2. Of those that a mesh axis runs over, the one named last changes fastest.
Arguments:
- skip_connection_stream: bfloat16 [4, 1024, 2048], P('dp', 'sp'), may hold values from -6 to 6
- emitted_valve_unscaled: bfloat16 [4, 1024, 1024], P('dp', 'sp'), may hold values from -6 to 6
- channel_source_mapped: bfloat16 [4, 1024, 1024], P('dp', 'sp'), may hold values from -6 to 6
- hidden_source_mapped: bfloat16 [4, 1024, 256], P('dp', 'sp'), may hold values from -6 to 6
- probe_mapped_values: bfloat16 [4, 1024, 256], P('dp', 'sp'), may hold values from -6 to 6
- increment_premapped: float32 [4, 1024, 16], P('dp', None, 'sp'), may hold values from -6 to 6
- extra_log_fading: float32 [4, 1024, 16], P('dp', None, 'sp'), may hold values from -2 to 0
- channel_fading_speed: float32 [16], replicated, may hold values from 0 to 1, as said below
- channel_source_kernel: float32 [4, 1024], replicated, may hold values from -3 to 3
- hidden_source_kernel: float32 [4, 256], replicated, may hold values from -3 to 3
- probe_kernel_coefficients: float32 [4, 256], replicated, may hold values from -3 to 3
- cluster_scaling_factor: float32 [1024], replicated, may hold values from 0.1 to 1.9
- emitted_mapping_matrix: bfloat16 [1024, 2048], replicated, may hold values from -0.1875 to 0.1875
- standardize_scaling: float32 [2048], replicated, may hold values from 0.1 to 1.9
- standardize_offset: float32 [2048], replicated, may hold values from -2 to 2
- chosen_specialist_ids: int32 [4, 1024, 2], P('dp', 'sp'), may hold values from 0 to 7, all different within a row; in each aligned block of 128 rows (0 to 127, 128 to 255, ..., all dimensions but the last counted through in order) at most 48 rows name the same one
- specialist_mixing_shares: float32 [4, 1024, 2], P('dp', 'sp'), may hold values from 0.2 to 1
- specialist_gating_matrices: bfloat16 [8, 2048, 5120], P('sp', None, 'dp'), may hold values from -0.125 to 0.125
- raising_matrices: bfloat16 [8, 2048, 5120], P('sp', None, 'dp'), may hold values from -0.125 to 0.125
- lowering_matrices: bfloat16 [8, 5120, 2048], P('sp', 'dp'), may hold values from -0.078125 to 0.078125
Outputs:
- layer_out: bfloat16 [4, 1024, 2048], P('dp', 'sp')
The draws below stay inside these ranges and needn't reach their ends.
Inputs may be any that keep to these rules, and one draw needn't show every extreme that they name: `chosen_specialist_ids`: each row names two different experts. The rows of one device name no expert more than 48 times, a bound that some block reaches. `channel_fading_speed`: Positive.
All inputs are finite; a program needn't handle non-finite values.
Results may differ from the reference program's by a relative error of at most 0.015.
Values may be sent and summed in bfloat16 or wider, within the bound.
A program may use at most 128 MiB of HBM per device.

```python
import math
import jax
import jax.numpy as jnp
import numpy as np
from jax import lax

D = 2048
HEADS = 16
HEAD_DIM = 64
GROUPS = 4
STATE = 64
FF = 5120
KERNEL = 4
BLK = 128
TOK = 128
INNER = 1024
EXPERTS = 8
CAP = 48
FF_PART = 1280
LEN = 1024
BATCH = 4
N_SP = 8
N_DP = 4


def draw_increment_premapped(key, part):
    noise_key, shift_key = jax.random.split(key)
    block_count = LEN // TOK
    shifted = jax.random.uniform(shift_key, (BATCH, block_count, 1, HEADS), jnp.float32, -1.2, 1.2)
    noise = jax.random.normal(noise_key, (BATCH, block_count, TOK, HEADS), jnp.float32)
    return jnp.clip(noise + shifted, -6.0, 6.0).reshape(BATCH, LEN, HEADS)


def draw_extra_log_fading(key, part):
    spot_key, loss_key = jax.random.split(key)
    spots = jax.random.randint(spot_key, (BATCH, 1, HEADS, 2), 0, LEN)
    losses = jax.random.uniform(loss_key, (BATCH, 1, HEADS, 2), jnp.float32, 0.2, 0.5)
    matched = jnp.arange(LEN)[None, :, None, None] == spots
    return jnp.sum(jnp.where(matched, jnp.log(1.0 - losses), 0.0), axis=3)


def draw_channel_fading_speed(key, part):
    pick_key, fast_key, slow_key = jax.random.split(key, 3)
    fast_share = 0.5
    quick = jax.random.bernoulli(pick_key, fast_share, (HEADS,))
    fast_rate = jnp.exp(jax.random.uniform(fast_key, (HEADS,), jnp.float32, math.log(0.03), math.log(0.1))) / 0.8
    slow_rate = jnp.exp(jax.random.uniform(slow_key, (HEADS,), jnp.float32, math.log(0.2), math.log(0.8))) / (0.8 * LEN)
    return jnp.where(quick, fast_rate, slow_rate)


def block_scale(rng, extent, cuts, least, high):
    def one(dim, blocks):
        heights = jax.random.uniform(jax.random.fold_in(jax.random.fold_in(rng, 6), dim), (blocks,), jnp.float32, least / len(cuts), high / len(cuts))
        return jnp.repeat(jnp.exp(heights), extent[dim] // blocks).reshape((-1,) + (1,) * (len(extent) - dim - 1))

    gain = one(*cuts[0])
    for cut in cuts[1:]:
        gain = gain * one(*cut)
    return gain


def deal_out(stream_key, own, number, rows, number_of, top, reach, skew):
    sequence = jax.random.permutation(stream_key, number_of)
    crowded, common = portions_of(number_of, rows * top, reach, skew, True), portions_of(number_of, rows * top, reach, skew, False)
    places = jnp.arange(number_of)

    def named(lengths, rotation):
        used = int((lengths > 0).sum())
        fixed = max(1, used // 4)
        passed = fixed + (places - fixed + rotation * (used - fixed)) % max(1, number_of - fixed)
        return jnp.zeros((number_of,), jnp.int32).at[sequence[jnp.where(places < fixed, places, passed)]].set(jnp.asarray(lengths, jnp.int32))

    lengths = jnp.where(number % 4 == 0, named(crowded, number // 4), named(common, number - number // 4 - 1))
    mixed = jax.random.permutation(jax.random.fold_in(own, 3), number_of)
    donor, taker = mixed[0:number_of // 2 * 2:2], mixed[1:number_of // 2 * 2:2]
    room = jnp.minimum(lengths[donor] - 1, reach - lengths[taker]) // 2
    room = jnp.where((donor == sequence[0]) | (taker == sequence[0]) | (lengths[taker] == 0), 0, jnp.maximum(room, 0))
    passed = jax.random.randint(jax.random.fold_in(own, 4), (number_of // 2,), 0, 1 << 20) % (room + 1)
    lengths = lengths.at[donor].add(-passed).at[taker].add(passed)
    members = jnp.searchsorted(jnp.cumsum(lengths), jnp.arange(rows * top), side="right").astype(jnp.int32)
    grid = members.reshape(top, rows).T
    grid = grid[jax.random.permutation(jax.random.fold_in(own, 1), rows)]
    rotation = jax.random.randint(jax.random.fold_in(own, 2), (rows, 1), 0, top)
    return jnp.take_along_axis(grid, (jnp.arange(top)[None, :] + rotation) % top, axis=1)


def portions_of(amount, total, limit, lean, full):
    loads = [(1 << 20) // math.isqrt(grade ** lean) + 1 for grade in range(1, amount + 1)]
    largest = limit if full else min(limit, max(-(-total // amount), total * loads[0] // sum(loads)))
    least = 1 if total - largest >= amount - 1 else 0
    given, rest = [largest] + [least] * (amount - 1), total - largest - least * (amount - 1)
    while rest > 0:
        free = [i for i in range(1, amount) if given[i] < largest] or [i for i in range(1, amount) if given[i] < limit]
        whole, left = sum([loads[i] for i in free]), rest
        for i in free:
            more = min(limit - given[i], max(1, left * loads[i] // whole), rest)
            given[i] = given[i] + more
            rest = rest - more
    return np.array(given)


def bell_draw(rng, dims, scale, limit, cuts=(), held_as=jnp.bfloat16):
    array = scale * jax.random.normal(rng, dims, jnp.float32)
    if cuts:
        array = array * block_scale(rng, dims, cuts, -0.22, 0.18)
    return jnp.clip(array, -limit, limit).astype(held_as)


def setup_inputs(seed: int = 0) -> dict:
    key_list = jax.random.split(jax.random.key(seed), 21)
    skip_connection_stream = bell_draw(key_list[0], (BATCH, LEN, D), 1.0, 6.0, ((0, 4), (1, 8)))
    emitted_valve_unscaled = bell_draw(key_list[1], (BATCH, LEN, INNER), 1.0, 6.0, ((0, 4), (1, 8)))
    channel_source_mapped = bell_draw(key_list[2], (BATCH, LEN, INNER), 1.0, 6.0, ((0, 4), (1, 8)))
    hidden_source_mapped = bell_draw(key_list[3], (BATCH, LEN, GROUPS * STATE), 1.0, 6.0, ((0, 4), (1, 8)))
    probe_mapped_values = bell_draw(key_list[4], (BATCH, LEN, GROUPS * STATE), 1.0, 6.0, ((0, 4), (1, 8)))
    increment_premapped = draw_increment_premapped(jax.random.fold_in(key_list[20], 71), 0)
    extra_log_fading = draw_extra_log_fading(jax.random.fold_in(key_list[20], 71), 0)
    channel_fading_speed = draw_channel_fading_speed(jax.random.fold_in(key_list[20], 71), 0)
    channel_source_kernel = bell_draw(key_list[8], (KERNEL, INNER), KERNEL ** -0.5, 3.0, (), jnp.float32)
    hidden_source_kernel = bell_draw(key_list[9], (KERNEL, GROUPS * STATE), KERNEL ** -0.5, 3.0, (), jnp.float32)
    probe_kernel_coefficients = bell_draw(key_list[10], (KERNEL, GROUPS * STATE), KERNEL ** -0.5, 3.0, (), jnp.float32)
    cluster_scaling_factor = jnp.clip(1.0 + 0.18 * jax.random.normal(key_list[11], (INNER,), jnp.float32), 0.1, 1.9)
    emitted_mapping_matrix = bell_draw(key_list[12], (INNER, D), INNER ** -0.5, 0.1875)
    standardize_scaling = jnp.clip(1.0 + 0.18 * jax.random.normal(key_list[13], (D,), jnp.float32), 0.1, 1.9)
    standardize_offset = bell_draw(key_list[14], (D,), 0.3, 2.0, (), jnp.float32)
    chosen_specialist_ids_keys = jax.random.split(jax.random.fold_in(key_list[15], 1), BATCH * LEN // TOK)
    chosen_specialist_ids_turns = jax.random.permutation(jax.random.fold_in(key_list[15], 3), BATCH * LEN // TOK)
    chosen_specialist_ids = jax.vmap(lambda own, number: deal_out(jax.random.fold_in(key_list[15], 2), own, number, TOK, EXPERTS, 2, CAP, 2))(chosen_specialist_ids_keys, chosen_specialist_ids_turns).reshape((BATCH, LEN, 2))
    specialist_mixing_shares = jnp.clip(0.2 + 0.8 * jax.random.uniform(key_list[16], (BATCH, LEN, 2), jnp.float32) ** block_scale(key_list[16], (BATCH, LEN, 2), ((0, 4), (1, 8)), -0.2, 0.2), 0.2, 1.0)
    specialist_gating_matrices = bell_draw(key_list[17], (EXPERTS, D, FF), D ** -0.5, 0.125, ((0, 8), (2, 4)))
    raising_matrices = bell_draw(key_list[18], (EXPERTS, D, FF), D ** -0.5, 0.125, ((0, 8), (2, 4)))
    lowering_matrices = bell_draw(key_list[19], (EXPERTS, FF, D), FF ** -0.5, 0.078125, ((0, 8), (1, 4)))
    return dict(skip_connection_stream=skip_connection_stream, emitted_valve_unscaled=emitted_valve_unscaled, channel_source_mapped=channel_source_mapped, hidden_source_mapped=hidden_source_mapped, probe_mapped_values=probe_mapped_values, increment_premapped=increment_premapped, extra_log_fading=extra_log_fading, channel_fading_speed=channel_fading_speed, channel_source_kernel=channel_source_kernel, hidden_source_kernel=hidden_source_kernel, probe_kernel_coefficients=probe_kernel_coefficients, cluster_scaling_factor=cluster_scaling_factor, emitted_mapping_matrix=emitted_mapping_matrix, standardize_scaling=standardize_scaling, standardize_offset=standardize_offset, chosen_specialist_ids=chosen_specialist_ids, specialist_mixing_shares=specialist_mixing_shares, specialist_gating_matrices=specialist_gating_matrices, raising_matrices=raising_matrices, lowering_matrices=lowering_matrices)


rms_eps = 1e-06
norm_eps = 1e-05

def causal_conv(series, tap_weights, rim_rows):
    padded = jnp.concatenate([rim_rows, series], axis=0).astype(jnp.float32)
    length = series.shape[0]
    running = jnp.zeros(series.shape, jnp.float32)
    for tap_index in range(tap_weights.shape[0]):
        running = running + tap_weights[tap_index].astype(jnp.float32) * lax.slice_in_dim(padded, tap_index, tap_index + length, axis=0)
    return jax.nn.silu(running).astype(jnp.bfloat16)

def ssd_blocks(x_conv, b_conv, c_conv, increment_delta, fading_exponent, init_state, block_len):
    length, head_count, head_width = x_conv.shape
    state_width = b_conv.shape[2]
    block_count = length // block_len
    x_block = x_conv.reshape(block_count, block_len, head_count, head_width).astype(jnp.float32)
    b_block = b_conv.reshape(block_count, block_len, head_count, state_width).astype(jnp.float32)
    c_block = c_conv.reshape(block_count, block_len, head_count, state_width).astype(jnp.float32)
    cumulative = jnp.cumsum(jnp.transpose(fading_exponent.reshape(block_count, block_len, head_count), (0, 2, 1)), axis=2)
    step_heads = jnp.transpose(increment_delta.reshape(block_count, block_len, head_count), (0, 2, 1))
    causal = jnp.arange(block_len)[:, None] >= jnp.arange(block_len)[None, :]
    within = jnp.exp(jnp.where(causal, cumulative[:, :, :, None] - cumulative[:, :, None, :], -jnp.inf))
    scores = jnp.einsum('cthn,cshn->chts', c_block, b_block)
    mixing = (scores * within * step_heads[:, :, None, :]).astype(jnp.bfloat16)
    diag_out = jnp.einsum('chts,cshp->cthp', mixing.astype(jnp.float32), x_block)
    tail_decay = jnp.exp(cumulative[:, :, -1:] - cumulative) * step_heads
    scaled = (x_block * jnp.transpose(tail_decay, (0, 2, 1))[:, :, :, None]).astype(jnp.bfloat16)
    block_state = jnp.einsum('cshp,cshn->chpn', scaled.astype(jnp.float32), b_block)
    totals = cumulative[:, :, -1]
    through = jnp.cumsum(totals, axis=0)
    before = through - totals
    earlier = jnp.arange(block_count)[:, None] > jnp.arange(block_count)[None, :]
    carry_weight = jnp.exp(jnp.where(earlier[:, :, None], before[:, None, :] - through[None, :, :], -jnp.inf))
    entering = jnp.einsum('cjh,jhpn->chpn', carry_weight, block_state, precision=lax.Precision.HIGHEST) + jnp.exp(before)[:, :, None, None] * init_state[None]
    reach_decay = jnp.transpose(jnp.exp(cumulative), (0, 2, 1))
    carried_out = jnp.einsum('cthn,chpn->cthp', c_block, entering, precision=lax.Precision.HIGHEST) * reach_decay[:, :, :, None]
    outcome = (diag_out + carried_out).reshape(length, head_count, head_width)
    final_state = jnp.einsum('jh,jhpn->hpn', jnp.exp(through[-1][None, :] - through), block_state, precision=lax.Precision.HIGHEST) + jnp.exp(through[-1])[:, None, None] * init_state
    return (outcome, final_state, through[-1])

def reference(skip_connection_stream, emitted_valve_unscaled, channel_source_mapped, hidden_source_mapped, probe_mapped_values, increment_premapped, extra_log_fading, channel_fading_speed, channel_source_kernel, hidden_source_kernel, probe_kernel_coefficients, cluster_scaling_factor, emitted_mapping_matrix, standardize_scaling, standardize_offset, chosen_specialist_ids, specialist_mixing_shares, specialist_gating_matrices, raising_matrices, lowering_matrices):
    per_group = HEADS // GROUPS
    tap_weights = jnp.concatenate([channel_source_kernel, hidden_source_kernel, probe_kernel_coefficients], axis=1)

    def lone_token_list(token_segments):
        channel_source_list, hidden_source_list, probe_value_list, increment_list, extra_fading_list = token_segments
        joined_rows = jnp.concatenate([channel_source_list, hidden_source_list, probe_value_list], axis=1)
        rim_rows = jnp.zeros((KERNEL - 1, joined_rows.shape[1]), jnp.bfloat16)
        convolved = causal_conv(joined_rows, tap_weights, rim_rows)
        x_conv = convolved[:, :INNER].reshape(LEN, HEADS, HEAD_DIM)
        b_conv = jnp.repeat(convolved[:, INNER:INNER + GROUPS * STATE].reshape(LEN, GROUPS, STATE), per_group, axis=1)
        c_conv = jnp.repeat(convolved[:, INNER + GROUPS * STATE:].reshape(LEN, GROUPS, STATE), per_group, axis=1)
        increment_delta = jax.nn.softplus(increment_list)
        fading_exponent = extra_fading_list - channel_fading_speed[None, :] * increment_delta
        init_state = jnp.zeros((HEADS, HEAD_DIM, STATE), jnp.float32)
        outcome, final_state, total_decay = ssd_blocks(x_conv, b_conv, c_conv, increment_delta, fading_exponent, init_state, BLK)
        return outcome.reshape(LEN, INNER).astype(jnp.bfloat16)
    blending_outcome = lax.map(lone_token_list, (channel_source_mapped, hidden_source_mapped, probe_mapped_values, increment_premapped, extra_log_fading))
    all_rows = BATCH * LEN
    gated = blending_outcome.reshape(all_rows, INNER).astype(jnp.float32) * jax.nn.silu(emitted_valve_unscaled.reshape(all_rows, INNER).astype(jnp.float32))
    grouped = gated.reshape(all_rows, GROUPS, INNER // GROUPS)
    grouped = grouped * lax.rsqrt(lax.optimization_barrier(jnp.mean(grouped * grouped, axis=-1, keepdims=True)) + rms_eps)
    group_normed = (grouped.reshape(all_rows, INNER) * cluster_scaling_factor[None, :]).astype(jnp.bfloat16)
    pre_norm = skip_connection_stream.reshape(all_rows, D).astype(jnp.float32) + jnp.dot(group_normed, emitted_mapping_matrix, preferred_element_type=jnp.float32)
    centre = lax.optimization_barrier(jnp.mean(pre_norm, axis=-1, keepdims=True))
    variance = lax.optimization_barrier(jnp.mean(jnp.square(pre_norm - centre), axis=-1, keepdims=True))
    normed = ((pre_norm - centre) * lax.rsqrt(variance + norm_eps) * standardize_scaling[None, :] + standardize_offset[None, :]).astype(jnp.bfloat16)
    flat_ids = chosen_specialist_ids.reshape(-1).astype(jnp.int32)
    flat_weights = specialist_mixing_shares.reshape(-1).astype(jnp.float32)
    owner = (jnp.arange(all_rows * 2, dtype=jnp.int32) // 2).astype(jnp.int32)
    buffer_rows = N_SP * N_DP * CAP
    padded_rows = jnp.concatenate([normed, jnp.zeros((1, D), jnp.bfloat16)], axis=0)

    def one_expert(running, expert):
        matched = flat_ids == expert
        ranked = jnp.cumsum(matched.astype(jnp.int32)) - 1
        placed = jnp.where(matched, ranked, buffer_rows).astype(jnp.int32)
        source = jnp.full((buffer_rows + 1,), all_rows, jnp.int32).at[placed].set(owner)[:buffer_rows]
        weight_at = jnp.zeros((buffer_rows + 1,), jnp.float32).at[placed].set(flat_weights)[:buffer_rows]
        rows_in = padded_rows[source]
        gate_val = jnp.dot(rows_in, specialist_gating_matrices[expert], preferred_element_type=jnp.float32)
        up_val = jnp.dot(rows_in, raising_matrices[expert], preferred_element_type=jnp.float32)
        hidden = (jax.nn.silu(gate_val) * up_val).astype(jnp.bfloat16)
        expert_sum = jnp.zeros((buffer_rows, D), jnp.float32)
        for part_index in range(N_DP):
            lower = part_index * FF_PART
            partial_value = jnp.dot(hidden[:, lower:lower + FF_PART], lowering_matrices[expert, lower:lower + FF_PART], preferred_element_type=jnp.float32).astype(jnp.bfloat16)
            expert_sum = expert_sum + lax.optimization_barrier(partial_value).astype(jnp.float32)
        expert_out = expert_sum.astype(jnp.bfloat16)
        running = running.at[source].add(weight_at[:, None] * expert_out.astype(jnp.float32))
        return (running, None)
    routed_sum, unused = lax.scan(one_expert, jnp.zeros((all_rows + 1, D), jnp.float32), jnp.arange(EXPERTS, dtype=jnp.int32))
    layer_out = (normed.astype(jnp.float32) + routed_sum[:all_rows]).astype(jnp.bfloat16)
    return layer_out.reshape(BATCH, LEN, D)
```

```python
import functools

import jax
import jax.numpy as jnp
from jax import lax
from jax.experimental import pallas as pl
from jax.experimental.pallas import tpu as pltpu
from jax.sharding import PartitionSpec as P

HEADS = 16
HEAD_DIM = 64
GROUPS = 4
STATE = 64
KERNEL = 4
BLK = 128

RMS_EPS = 1e-06
NORM_EPS = 1e-05
HALO = 16
MESH = pl.DeviceIdType.MESH
F32 = jnp.float32
BF16 = jnp.bfloat16
I32 = jnp.int32


def flip(value, mask):
    result, bit = value, 1
    while bit <= mask:
        if mask & bit:
            result = result + bit * (1 - 2 * ((value // bit) % 2))
        bit *= 2
    return result


def iota(shape, dim):
    return lax.broadcasted_iota(I32, shape, dim)


def lane_scan(value, width):
    lanes = iota(value.shape, 1)
    step = 1
    while step < width:
        value = value + jnp.where(lanes >= step, pltpu.roll(value, step, 1), 0.0)
        step *= 2
    return value


def layer_kernel(
    S, R, Y, cap,
    xs_hbm, bs_hbm, cs_hbm, valve_hbm, skip_hbm, wo_hbm, wg_hbm, wu_hbm, wd_hbm,
    inc_ref, fade_ref, speed_ref, xk_ref, bk_ref, ck_ref, gain_ref, lns_ref, lno_ref,
    ids_ref, share_ref,
    out_ref,
    joined, conv, valve, skip, wo, msg, rbuf, step_rows, decay_rows, total_rows, rows, cols,
    cmask, diag, scaled, state, sendz, recvz, sendy, recvy, normed_g, pre, normed,
    outb, arr, hid, ra, rx, sx, ret, wg, wu, wd,
    in_sem, w_sem, m_s, m_r, h_s, h_r, z_s, z_r, y_s, y_r,
    d_s, d_r, g_s, g_r, a_s, a_r, x_s, x_r, b_s, b_r,
):
    s = lax.axis_index("sp")
    d = lax.axis_index("dp")
    T, inner = xs_hbm.shape
    span = bs_hbm.shape[1]
    width = skip_hbm.shape[1]
    ff = wg_hbm.shape[1]
    hc = inc_ref.shape[0]
    H = HEADS
    G = GROUPS
    gw = inner // G
    pair = 2 * HEAD_DIM
    zi = s // Y
    yi = s % Y
    Z = S // Y
    nx = R // 2

    def remote(src, dst, send, recv, where):
        return pltpu.make_async_remote_copy(
            src_ref=src, dst_ref=dst, send_sem=send, recv_sem=recv,
            device_id=where, device_id_type=MESH,
        )

    def local(src, dst, sem):
        return pltpu.make_async_copy(src, dst, sem)

    body = pl.ds(HALO, T)
    loads = [
        local(xs_hbm, joined.at[body, pl.ds(0, inner)], in_sem.at[0]),
        local(bs_hbm, joined.at[body, pl.ds(inner, span)], in_sem.at[1]),
        local(cs_hbm, joined.at[body, pl.ds(inner + span, span)], in_sem.at[2]),
        local(valve_hbm, valve, in_sem.at[3]),
        local(skip_hbm, skip, in_sem.at[4]),
        local(wo_hbm, wo, in_sem.at[5]),
    ]
    weights = [
        local(src, dst, w_sem.at[i])
        for i, (src, dst) in enumerate(((wg_hbm, wg), (wu_hbm, wu), (wd_hbm, wd)))
    ]
    for load in loads:
        load.start()

    barrier = pltpu.get_barrier_semaphore()
    peers = [{"sp": flip(s, j)} for j in range(1, S)]
    peers += [{"dp": flip(d, 1)}] + [{"dp": flip(d, 2 * dx)} for dx in range(1, nx)]
    for peer in peers:
        pl.semaphore_signal(barrier, inc=1, device_id=peer, device_id_type=MESH)

    step_in = jax.nn.softplus(inc_ref[...])
    own_rows = iota((hc, 1), 0)
    speeds = jnp.zeros((hc, 1), F32)
    for i in range(hc):
        speeds = jnp.where(own_rows == i, speed_ref[s * hc + i], speeds)
    decay_in = fade_ref[...] - speeds * step_in
    tot_lanes = iota((hc, T), 1)
    totals_in = jnp.zeros((hc, T), F32)
    for j in range(S):
        block = decay_in[:, j * T : (j + 1) * T]
        totals_in = jnp.where(tot_lanes == j, jnp.sum(block, axis=1, keepdims=True), totals_in)
    for j in range(S):
        msg[j, pl.ds(0, hc), :] = step_in[:, j * T : (j + 1) * T]
        msg[j, pl.ds(hc, hc), :] = decay_in[:, j * T : (j + 1) * T]
        msg[j, pl.ds(2 * hc, hc), :] = totals_in
        msg[j, pl.ds(3 * hc, 8 - 3 * hc), :] = jnp.zeros((8 - 3 * hc, T), F32)

    pl.semaphore_wait(barrier, len(peers))

    def share_steps(j):
        return remote(msg.at[flip(s, j)], rbuf.at[s], m_s.at[j], m_r.at[j], {"sp": flip(s, j)})

    def halo_to():
        return remote(
            joined.at[pl.ds(T, HALO)], joined.at[pl.ds(0, HALO)], h_s, h_r, {"sp": s + 1}
        )

    for j in range(S - 1, 0, -1):
        share_steps(j).start()
    rbuf[s] = msg[s]

    for load in loads[:3]:
        load.wait()

    @pl.when(s < S - 1)
    def _():
        halo_to().start()

    for load in weights:
        load.start()

    @pl.when(s == 0)
    def _():
        joined[pl.ds(0, HALO), :] = jnp.zeros((HALO, joined.shape[1]), BF16)

    @pl.when(zi == 0)
    def _():
        recvz[...] = jnp.zeros(recvz.shape, BF16)

    experts = iota((S, T), 0)
    hot = [(ids_ref[k : k + 1, :] == experts) for k in range(2)]
    named = (hot[0].astype(F32) + hot[1].astype(F32)).astype(BF16)
    before_t = (iota((T, T), 0) < iota((T, T), 1)).astype(F32).astype(BF16)
    ranks = jnp.dot(named, before_t, preferred_element_type=F32)
    targets = []
    for k in range(2):
        rank = jnp.sum(jnp.where(hot[k], ranks, 0.0), axis=0, keepdims=True)
        relative = jnp.bitwise_xor(ids_ref[k : k + 1, :], s)
        targets.append(relative * cap + rank.astype(I32))
        rows[3 * H + k : 3 * H + k + 1, :] = targets[k].astype(F32)
    rows[3 * H + 2 :, :] = jnp.zeros((rows.shape[0] - 3 * H - 2, T), F32)

    @pl.when(s > 0)
    def _():
        halo_to().wait_recv()

    chunk = 256
    first = HALO - KERNEL + 1
    for taps, at in ((xk_ref, 0), (bk_ref, inner), (ck_ref, inner + span)):
        for c in range(0, taps.shape[1], chunk):
            series = joined[:, at + c : at + c + chunk].astype(F32)
            total = jnp.zeros((T, chunk), F32)
            for k in range(KERNEL):
                total = total + taps[k : k + 1, c : c + chunk] * series[first + k : first + k + T, :]
            conv[:, at + c : at + c + chunk] = jax.nn.silu(total).astype(BF16)

    for j in range(1, S):
        share_steps(j).wait_recv()
    for p in range(S):
        at = pl.ds(p * hc, hc)
        step_rows[at, :] = rbuf[p, pl.ds(0, hc), :]
        decay_rows[at, :] = rbuf[p, pl.ds(hc, hc), :]
        total_rows[at, :] = rbuf[p, pl.ds(2 * hc, hc), :]
    steps = step_rows[...]
    cumulative = lane_scan(decay_rows[...], T)
    final = jnp.sum(jnp.where(iota((H, T), 1) == T - 1, cumulative, 0.0), axis=1, keepdims=True)
    rows[0:H, :] = cumulative
    rows[H : 2 * H, :] = jnp.exp(final - cumulative) * steps
    rows[2 * H : 3 * H, :] = jnp.exp(cumulative)
    cols[...] = rows[...].T

    lane = iota((T, pair), 1)
    low = lane < HEAD_DIM

    def by_head(base, q):
        return jnp.where(
            low, cols[:, base + 2 * q : base + 2 * q + 1], cols[:, base + 2 * q + 1 : base + 2 * q + 2]
        )

    for q in range(H // 2):
        at = pl.ds(q * pair, pair)
        scaled[:, at] = (conv[:, at].astype(F32) * by_head(H, q)).astype(BF16)
    for p in range(G // 2):
        b_pair = conv[:, inner + p * pair : inner + (p + 1) * pair]
        both = lax.dot_general(
            b_pair, scaled[:, 2 * gw * p : 2 * gw * (p + 1)], (((0,), (0,)), ((), ())),
            preferred_element_type=F32,
        )
        for i in range(2):
            state[2 * p + i] = both[i * STATE : (i + 1) * STATE, i * gw : (i + 1) * gw]

    lanes_h = iota((H, T), 1)
    through = lane_scan(total_rows[...], S)
    ahead_of = through - total_rows[...]

    def pick(values, index):
        return jnp.sum(jnp.where(lanes_h == index, values, 0.0), axis=1, keepdims=True)

    head_of = iota((H, inner), 1) // HEAD_DIM == iota((H, inner), 0)

    def spread(column):
        return jnp.sum(jnp.where(head_of, column, 0.0), axis=0, keepdims=True)

    at_plane = pick(ahead_of, zi * Y)
    at_next = pick(ahead_of, zi * Y + Y)
    at_here = pick(ahead_of, s)
    past_here = pick(through, s)
    zf = spread(jnp.exp(at_next - at_plane))
    zs = spread(jnp.exp(at_next - past_here))
    own_f = spread(jnp.exp(at_here - at_plane))
    yf, ys = [None], [None]
    for dy in range(1, Y):
        at_peer = pick(ahead_of, flip(s, dy))
        later = flip(s, dy) > s
        yf.append(spread(jnp.exp(at_peer - at_plane)))
        ys.append(spread(jnp.where(later, jnp.exp(jnp.minimum(at_peer - past_here, 0.0)), 0.0)))

    def column(values, g):
        return values[:, g * gw : (g + 1) * gw]

    def along_z(g):
        return remote(sendz.at[g], recvz.at[g], z_s.at[g], z_r.at[g], {"sp": s + Y})

    def along_y(dy, g):
        return remote(
            sendy.at[dy - 1, g], recvy.at[dy - 1, g], y_s.at[dy - 1, g], y_r.at[dy - 1, g],
            {"sp": flip(s, dy)},
        )

    @pl.when(zi == 0)
    def _():
        for g in range(G):
            sendz[g] = (column(zs, g) * state[g]).astype(BF16)
            along_z(g).start()

    causal = iota((T, T), 0) >= iota((T, T), 1)
    for g in range(G):
        p, i = g // 2, g % 2
        at_b = inner + p * pair
        at_c = inner + span + p * pair
        half = low if i == 0 else jnp.logical_not(low)
        c_half = jnp.where(half, conv[:, at_c : at_c + pair].astype(F32), 0.0).astype(BF16)
        cmask[g] = c_half
        scores = lax.dot_general(
            c_half, conv[:, at_b : at_b + pair], (((1,), (1,)), ((), ())),
            preferred_element_type=F32,
        )
        per = H // G // 2
        for q in range(g * per, (g + 1) * per):
            at = pl.ds(q * pair, pair)
            mixes = []
            for h in (2 * q, 2 * q + 1):
                gap = jnp.where(causal, cols[:, h : h + 1] - rows[h : h + 1, :], -jnp.inf)
                mixes.append((scores * jnp.exp(gap) * step_rows[h : h + 1, :]).astype(BF16))
            x_pair = conv[:, at].astype(F32)
            stacked = jnp.concatenate(
                [jnp.where(low, x_pair, 0.0).astype(BF16), jnp.where(low, 0.0, x_pair).astype(BF16)],
                axis=0,
            )
            diag[:, at] = jnp.dot(
                jnp.concatenate(mixes, axis=1), stacked, preferred_element_type=F32
            )

    for g in range(G):
        @pl.when(zi > 0)
        def _():
            along_z(g).wait_recv()

        @pl.when(jnp.logical_and(zi > 0, zi < Z - 1))
        def _():
            sendz[g] = (column(zf, g) * recvz[g].astype(F32) + column(zs, g) * state[g]).astype(BF16)
            along_z(g).start()

        for dy in range(1, Y):
            sendy[dy - 1, g] = (
                column(yf[dy], g) * recvz[g].astype(F32) + column(ys[dy], g) * state[g]
            ).astype(BF16)
            along_y(dy, g).start()

    for load in loads[3:]:
        load.wait()
    for g in range(G):
        at = pl.ds(g * gw, gw)
        entering = column(own_f, g) * recvz[g].astype(F32)
        for dy in range(1, Y):
            along_y(dy, g).wait_recv()
            entering = entering + recvy[dy - 1, g].astype(F32)
        high = entering.astype(BF16)
        rest = (entering - high.astype(F32)).astype(BF16)
        c_half = cmask[g]
        carried = jnp.dot(
            c_half, jnp.concatenate([high, high], axis=0), preferred_element_type=F32
        ) + jnp.dot(c_half, jnp.concatenate([rest, rest], axis=0), preferred_element_type=F32)
        per = H // G // 2
        reach = jnp.concatenate([by_head(2 * H, q) for q in range(g * per, (g + 1) * per)], axis=1)
        mixed = (diag[:, at] + carried * reach).astype(BF16)
        gated = mixed.astype(F32) * jax.nn.silu(valve[:, at].astype(F32))
        power = jnp.mean(gated * gated, axis=-1, keepdims=True)
        normed_g[:, at] = (gated * lax.rsqrt(power + RMS_EPS) * gain_ref[:, at]).astype(BF16)
        base = skip[...].astype(F32) if g == 0 else pre[...]
        pre[...] = base + jnp.dot(normed_g[:, at], wo[at, :], preferred_element_type=F32)

    tile = 16

    def normalise(i, carry):
        at = pl.ds(pl.multiple_of(i * tile, tile), tile)
        value = pre[at, :]
        centre = jnp.mean(value, axis=-1, keepdims=True)
        gap = value - centre
        variance = jnp.mean(gap * gap, axis=-1, keepdims=True)
        normed[at, :] = (
            gap * lax.rsqrt(variance + NORM_EPS) * lns_ref[...] + lno_ref[...]
        ).astype(BF16)
        return carry

    lax.fori_loop(0, T // tile, normalise, 0)

    order = list(range(S))
    ahead = 2

    def slot_rows(j, dc, dx, count=1):
        return pl.ds((j * R + dc * nx + dx) * cap, count * cap)

    def disp(j):
        return remote(outb.at[pl.ds(j * cap, cap)], arr.at[slot_rows(j, 0, 0)],
                      d_s.at[j], d_r.at[j], {"sp": flip(s, j)})

    def agx(j, dx):
        return remote(arr.at[slot_rows(j, 0, 0)], arr.at[slot_rows(j, 0, dx)],
                      g_s.at[j, dx], g_r.at[j, dx], {"dp": flip(d, 2 * dx)})

    def agc(j, dx):
        return remote(arr.at[slot_rows(j, 0, dx)], arr.at[slot_rows(j, 1, dx)],
                      g_s.at[j, nx + dx], g_r.at[j, nx + dx], {"dp": flip(d, 1)})

    def rsc(j):
        return remote(arr.at[slot_rows(j, 1, 0, nx)], ra.at[pl.ds(j * nx * cap, nx * cap)],
                      a_s.at[j], a_r.at[j], {"dp": flip(d, 1)})

    def rsx(j, dx):
        at = pl.ds((j * (nx - 1) + dx - 1) * cap, cap)
        return remote(sx.at[at], rx.at[at], x_s.at[j, dx], x_r.at[j, dx], {"dp": flip(d, 2 * dx)})

    def back(j):
        return remote(outb.at[pl.ds(j * cap, cap)], ret.at[pl.ds(j * cap, cap)],
                      b_s.at[j], b_r.at[j], {"sp": flip(s, j)})

    def place(j):
        slot = iota((cap, T), 0) + j * cap
        hit = jnp.logical_or(slot == targets[0], slot == targets[1])
        moved = jnp.dot(
            hit.astype(F32).astype(BF16), normed[...], preferred_element_type=F32
        ).astype(BF16)
        if j:
            outb[pl.ds(j * cap, cap), :] = moved
            disp(j).start()
        else:
            arr[slot_rows(0, 0, 0), :] = moved

    for j in order:
        place(j)

    def arrive(j):
        if j:
            disp(j).wait_recv()
        for dx in range(1, nx):
            agx(j, dx).start()
        agc(j, 0).start()

    def relay(j):
        for dx in range(1, nx):
            agx(j, dx).wait_recv()
            agc(j, dx).start()

    def gate_up(j):
        for dx in range(nx):
            agc(j, dx).wait_recv()
        wide = 256 if ff % 256 == 0 else 128

        def piece(i, carry):
            at = pl.ds(pl.multiple_of(i * wide, wide), wide)
            x = arr[slot_rows(j, 0, 0, R), :]
            g = jnp.dot(x, wg[:, at], preferred_element_type=F32)
            u = jnp.dot(x, wu[:, at], preferred_element_type=F32)
            hid[:, at] = (jax.nn.silu(g) * u).astype(BF16)
            return carry

        lax.fori_loop(0, ff // wide, piece, 0)

    def down(j):
        for dx in range(nx):
            if dx:
                agx(j, dx).wait_send()
            agc(j, dx).wait_send()
        wide = 256 if width % 256 == 0 else 128

        def piece(i, carry):
            at = pl.ds(pl.multiple_of(i * wide, wide), wide)
            arr[slot_rows(j, 0, 0, R), at] = jnp.dot(
                hid[...], wd[:, at], preferred_element_type=F32
            ).astype(BF16)
            return carry

        lax.fori_loop(0, width // wide, piece, 0)
        rsc(j).start()

    def chip_sum(j):
        rsc(j).wait_recv()
        for dx in range(1, nx):
            both = (
                arr[slot_rows(j, 0, dx), :].astype(F32)
                + ra[pl.ds((j * nx + dx) * cap, cap), :].astype(F32)
            )
            sx[pl.ds((j * (nx - 1) + dx - 1) * cap, cap), :] = both.astype(BF16)
            rsx(j, dx).start()

    def finish(j):
        total = (
            arr[slot_rows(j, 0, 0), :].astype(F32)
            + ra[pl.ds(j * nx * cap, cap), :].astype(F32)
        )
        for dx in range(1, nx):
            rsx(j, dx).wait_recv()
            total = total + rx[pl.ds((j * (nx - 1) + dx - 1) * cap, cap), :].astype(F32)
        if j:
            disp(j).wait_send()
            outb[pl.ds(j * cap, cap), :] = total.astype(BF16)
            back(j).start()
        else:
            ret[pl.ds(0, cap), :] = total.astype(BF16)

    for j in order[:ahead]:
        arrive(j)
    weights[0].wait()
    weights[1].wait()
    for p, j in enumerate(order):
        relay(j)
        gate_up(j)
        if p + ahead < S:
            arrive(order[p + ahead])
        if p == 0:
            weights[2].wait()
        if p > 1:
            finish(order[p - 2])
        if p:
            chip_sum(order[p - 1])
        down(j)
    if S > 1:
        finish(order[S - 2])
    chip_sum(order[S - 1])
    finish(order[S - 1])

    target_cols = [cols[:, 3 * H + k : 3 * H + k + 1].astype(I32) for k in range(2)]
    shares = [share_ref[:, k : k + 1] for k in range(2)]
    pre[...] = normed[...].astype(F32)
    for j in order:
        if j:
            back(j).wait_recv()
        slot = iota((T, cap), 1) + j * cap
        hit = jnp.logical_or(slot == target_cols[0], slot == target_cols[1])
        share = jnp.zeros((T, 1), F32)
        for k in range(2):
            inside = jnp.logical_and(target_cols[k] >= j * cap, target_cols[k] < (j + 1) * cap)
            share = share + jnp.where(inside, shares[k], 0.0)
        moved = jnp.dot(
            hit.astype(F32).astype(BF16), ret[pl.ds(j * cap, cap), :], preferred_element_type=F32
        )
        pre[...] = pre[...] + share * moved
    out_ref[...] = pre[...].astype(BF16)

    for j in range(1, S):
        share_steps(j).wait_send()

    @pl.when(s < S - 1)
    def _():
        halo_to().wait_send()

    @pl.when(zi < Z - 1)
    def _():
        for g in range(G):
            along_z(g).wait_send()

    for g in range(G):
        for dy in range(1, Y):
            along_y(dy, g).wait_send()
    for j in range(S):
        rsc(j).wait_send()
        for dx in range(1, nx):
            rsx(j, dx).wait_send()
        if j:
            back(j).wait_send()


def run_layer(S, R, cap, big, small):
    xs, bs, cs, valve, skip, wo, wg, wu, wd = big
    T, inner = xs.shape
    span = bs.shape[1]
    width = skip.shape[1]
    ff = wg.shape[1]
    nx = R // 2
    Y = 1
    while Y * Y * 4 <= S:
        Y *= 2
    gw = inner // GROUPS
    dma = pltpu.SemaphoreType.DMA
    vmem = pltpu.VMEM
    total = S * R * cap
    whole = inner + 2 * span
    return pl.pallas_call(
        functools.partial(layer_kernel, S, R, Y, cap),
        out_shape=jax.ShapeDtypeStruct((T, width), BF16),
        in_specs=[pl.BlockSpec(memory_space=pl.ANY)] * 9
        + [pl.BlockSpec(memory_space=pltpu.VMEM)] * 2
        + [pl.BlockSpec(memory_space=pltpu.SMEM)]
        + [pl.BlockSpec(memory_space=pltpu.VMEM)] * 8,
        out_specs=pl.BlockSpec(memory_space=pltpu.VMEM),
        scratch_shapes=[
            vmem((HALO + T, whole), BF16),
            vmem((T, whole), BF16),
            vmem((T, inner), BF16),
            vmem((T, width), BF16),
            vmem((inner, width), BF16),
            vmem((S, 8, T), F32),
            vmem((S, 8, T), F32),
            vmem((HEADS, T), F32),
            vmem((HEADS, T), F32),
            vmem((HEADS, T), F32),
            vmem((T, T), F32),
            vmem((T, T), F32),
            vmem((GROUPS, T, 2 * STATE), BF16),
            vmem((T, inner), F32),
            vmem((T, inner), BF16),
            vmem((GROUPS, STATE, gw), F32),
            vmem((GROUPS, STATE, gw), BF16),
            vmem((GROUPS, STATE, gw), BF16),
            vmem((Y - 1, GROUPS, STATE, gw), BF16),
            vmem((Y - 1, GROUPS, STATE, gw), BF16),
            vmem((T, inner), BF16),
            vmem((T, width), F32),
            vmem((T, width), BF16),
            vmem((S * cap, width), BF16),
            vmem((total, width), BF16),
            vmem((R * cap, ff), BF16),
            vmem((S * nx * cap, width), BF16),
            vmem((S * (nx - 1) * cap, width), BF16),
            vmem((S * (nx - 1) * cap, width), BF16),
            vmem((S * cap, width), BF16),
            vmem((width, ff), BF16),
            vmem((width, ff), BF16),
            vmem((ff, width), BF16),
            dma((6,)), dma((3,)),
            dma((S,)), dma((S,)),
            dma(()), dma(()),
            dma((GROUPS,)), dma((GROUPS,)),
            dma((Y - 1, GROUPS)), dma((Y - 1, GROUPS)),
            dma((S,)), dma((S,)),
            dma((S, R)), dma((S, R)),
            dma((S,)), dma((S,)),
            dma((S, nx)), dma((S, nx)),
            dma((S,)), dma((S,)),
        ],
        compiler_params=pltpu.CompilerParams(
            collective_id=0, has_side_effects=True, vmem_limit_bytes=62 * 1024 * 1024
        ),
        cost_estimate=pl.CostEstimate(
            flops=6 * total * width * ff, bytes_accessed=6 * width * ff, transcendentals=total * ff
        ),
    )(*big, *small)


def per_device(
    skip_connection_stream,
    emitted_valve_unscaled,
    channel_source_mapped,
    hidden_source_mapped,
    probe_mapped_values,
    increment_premapped,
    extra_log_fading,
    channel_fading_speed,
    channel_source_kernel,
    hidden_source_kernel,
    probe_kernel_coefficients,
    cluster_scaling_factor,
    emitted_mapping_matrix,
    standardize_scaling,
    standardize_offset,
    chosen_specialist_ids,
    specialist_mixing_shares,
    specialist_gating_matrices,
    raising_matrices,
    lowering_matrices,
):
    S = lax.axis_size("sp")
    R = lax.axis_size("dp")
    T = skip_connection_stream.shape[1]
    assert T == BLK
    cap = -(-(3 * T // S) // 16) * 16
    big = (
        channel_source_mapped[0], hidden_source_mapped[0], probe_mapped_values[0],
        emitted_valve_unscaled[0], skip_connection_stream[0], emitted_mapping_matrix,
        specialist_gating_matrices[0], raising_matrices[0], lowering_matrices[0],
    )
    small = (
        increment_premapped[0].T, extra_log_fading[0].T, channel_fading_speed,
        channel_source_kernel, hidden_source_kernel, probe_kernel_coefficients,
        cluster_scaling_factor[None, :], standardize_scaling[None, :], standardize_offset[None, :],
        chosen_specialist_ids[0].T, specialist_mixing_shares[0],
    )
    return run_layer(S, R, cap, big, small)[None]


def solution(mesh):
    placed = (
        P("dp", "sp", None),
        P("dp", "sp", None),
        P("dp", "sp", None),
        P("dp", "sp", None),
        P("dp", "sp", None),
        P("dp", None, "sp"),
        P("dp", None, "sp"),
        P(),
        P(),
        P(),
        P(),
        P(),
        P(),
        P(),
        P(),
        P("dp", "sp", None),
        P("dp", "sp", None),
        P("sp", None, "dp"),
        P("sp", None, "dp"),
        P("sp", "dp", None),
    )
    return jax.shard_map(
        per_device, mesh=mesh, in_specs=placed, out_specs=P("dp", "sp", None), check_vma=False
    )
```

```python
import functools
import math

import jax
import jax.numpy as jnp
from jax import lax
from jax.experimental import pallas as pl
from jax.experimental.pallas import tpu as pltpu
from jax.sharding import PartitionSpec as P

HEADS = 16
HEAD_DIM = 64
GROUPS = 4
STATE = 64
KERNEL = 4
BLK = 128

RMS_EPS = 1e-06
NORM_EPS = 1e-05
HALO = 16
MESH = pl.DeviceIdType.MESH
F32 = jnp.float32
BF16 = jnp.bfloat16
I32 = jnp.int32


def flip(value, mask):
    result, bit = value, 1
    while bit <= mask:
        if mask & bit:
            result = result + bit * (1 - 2 * ((value // bit) % 2))
        bit *= 2
    return result


def iota(shape, dim):
    return lax.broadcasted_iota(I32, shape, dim)


def lane_scan(value, width):
    lanes = iota(value.shape, 1)
    step = 1
    while step < width:
        value = value + jnp.where(lanes >= step, pltpu.roll(value, step, 1), 0.0)
        step *= 2
    return value


ISSUE_OF_8 = "5 6 2 3 7 4 1"
PLAN_OF_8 = """
A0 A5 A1 R5 A6 G5 D5 A2 R6 C5 G6 A7 A3 R2 D6 R0 G2 D2 R7 C2 G7 F5 R3 C6 R1 D7
G3 A4 C7 F2 D3 F6 G1 C3 R4 D1 G4 F7 D4 C4 F3 C1 G0 D0 F4 C0 F1 F0
"""


def expert_plan(S):
    if S == 8:
        return (
            [0] + [int(j) for j in ISSUE_OF_8.split()],
            [(word[0], int(word[1:])) for word in PLAN_OF_8.split()],
        )
    order = list(range(S))
    plan = [("A", j) for j in order[:2]]
    for p, j in enumerate(order):
        plan += [("R", j), ("G", j)]
        if p + 2 < S:
            plan.append(("A", order[p + 2]))
        if p > 1:
            plan.append(("F", order[p - 2]))
        if p:
            plan.append(("C", order[p - 1]))
        plan.append(("D", j))
    if S > 1:
        plan.append(("F", order[S - 2]))
    plan += [("C", order[S - 1]), ("F", order[S - 1])]
    return order, plan


def layer_kernel(
    S, R, Y, cap,
    xs_hbm, bs_hbm, cs_hbm, valve_hbm, skip_hbm, wo_hbm, wg_hbm, wu_hbm, wd_hbm,
    inc_ref, fade_ref, speed_ref, xk_ref, bk_ref, ck_ref, gain_ref, lns_ref, lno_ref,
    ids_ref, share_ref,
    out_ref,
    joined, conv, valve, skip, wo, msg, rbuf, step_rows, decay_rows, total_rows, rows, cols,
    cmask, diag, scaled, state, sendz, recvz, sendy, recvy, normed_g, pre, normed,
    outb, arr, hid, ra, rx, sx, ret, wg, wu, wd,
    in_sem, w_sem, m_s, m_r, h_s, h_r, z_s, z_r, y_s, y_r,
    d_s, d_r, g_s, g_r, a_s, a_r, x_s, x_r, b_s, b_r,
):
    s = lax.axis_index("sp")
    d = lax.axis_index("dp")
    T, inner = xs_hbm.shape
    span = bs_hbm.shape[1]
    width = skip_hbm.shape[1]
    ff = wg_hbm.shape[1]
    hc = inc_ref.shape[0]
    H = HEADS
    G = GROUPS
    gw = inner // G
    pair = 2 * HEAD_DIM
    zi = s // Y
    yi = s % Y
    Z = S // Y
    nx = R // 2

    def remote(src, dst, send, recv, where):
        return pltpu.make_async_remote_copy(
            src_ref=src, dst_ref=dst, send_sem=send, recv_sem=recv,
            device_id=where, device_id_type=MESH,
        )

    def local(src, dst, sem):
        return pltpu.make_async_copy(src, dst, sem)

    body = pl.ds(HALO, T)
    loads = [
        local(xs_hbm, joined.at[body, pl.ds(0, inner)], in_sem.at[0]),
        local(bs_hbm, joined.at[body, pl.ds(inner, span)], in_sem.at[1]),
        local(cs_hbm, joined.at[body, pl.ds(inner + span, span)], in_sem.at[2]),
        local(valve_hbm, valve, in_sem.at[3]),
        local(skip_hbm, skip, in_sem.at[4]),
        local(wo_hbm, wo, in_sem.at[5]),
    ]
    weights = [
        local(src, dst, w_sem.at[i])
        for i, (src, dst) in enumerate(((wg_hbm, wg), (wu_hbm, wu), (wd_hbm, wd)))
    ]
    for load in loads:
        load.start()

    barrier = pltpu.get_barrier_semaphore()
    peers = [{"sp": flip(s, j)} for j in range(1, S)]
    peers += [{"dp": flip(d, 1)}] + [{"dp": flip(d, 2 * dx)} for dx in range(1, nx)]
    for peer in peers:
        pl.semaphore_signal(barrier, inc=1, device_id=peer, device_id_type=MESH)

    step_in = jax.nn.softplus(inc_ref[...])
    own_rows = iota((hc, 1), 0)
    speeds = jnp.zeros((hc, 1), F32)
    for i in range(hc):
        speeds = jnp.where(own_rows == i, speed_ref[s * hc + i], speeds)
    decay_in = fade_ref[...] - speeds * step_in
    tot_lanes = iota((hc, T), 1)
    totals_in = jnp.zeros((hc, T), F32)
    for j in range(S):
        block = decay_in[:, j * T : (j + 1) * T]
        totals_in = jnp.where(tot_lanes == j, jnp.sum(block, axis=1, keepdims=True), totals_in)
    for j in range(S):
        msg[j, pl.ds(0, hc), :] = step_in[:, j * T : (j + 1) * T]
        msg[j, pl.ds(hc, hc), :] = decay_in[:, j * T : (j + 1) * T]
        msg[j, pl.ds(2 * hc, hc), :] = totals_in
        msg[j, pl.ds(3 * hc, 8 - 3 * hc), :] = jnp.zeros((8 - 3 * hc, T), F32)

    pl.semaphore_wait(barrier, len(peers))

    def share_steps(j):
        return remote(msg.at[flip(s, j)], rbuf.at[s], m_s.at[j], m_r.at[j], {"sp": flip(s, j)})

    def halo_to():
        return remote(
            joined.at[pl.ds(T, HALO)], joined.at[pl.ds(0, HALO)], h_s, h_r, {"sp": s + 1}
        )

    for j in range(S - 1, 0, -1):
        share_steps(j).start()
    rbuf[s] = msg[s]

    for load in loads[:3]:
        load.wait()

    @pl.when(s < S - 1)
    def _():
        halo_to().start()

    for load in weights:
        load.start()

    @pl.when(s == 0)
    def _():
        joined[pl.ds(0, HALO), :] = jnp.zeros((HALO, joined.shape[1]), BF16)

    @pl.when(zi == 0)
    def _():
        recvz[...] = jnp.zeros(recvz.shape, BF16)

    experts = iota((S, T), 0)
    hot = [(ids_ref[k : k + 1, :] == experts) for k in range(2)]
    named = (hot[0].astype(F32) + hot[1].astype(F32)).astype(BF16)
    before_t = (iota((T, T), 0) < iota((T, T), 1)).astype(F32).astype(BF16)
    ranks = jnp.dot(named, before_t, preferred_element_type=F32)
    targets = []
    for k in range(2):
        rank = jnp.sum(jnp.where(hot[k], ranks, 0.0), axis=0, keepdims=True)
        relative = jnp.bitwise_xor(ids_ref[k : k + 1, :], s)
        targets.append(relative * cap + rank.astype(I32))
        rows[3 * H + k : 3 * H + k + 1, :] = targets[k].astype(F32)
    rows[3 * H + 2 : 3 * H + 4, :] = share_ref[...]
    rows[3 * H + 4 :, :] = jnp.zeros((rows.shape[0] - 3 * H - 4, T), F32)

    @pl.when(s > 0)
    def _():
        halo_to().wait_recv()

    chunk = 256
    first = HALO - KERNEL + 1
    for taps, at in ((xk_ref, 0), (bk_ref, inner), (ck_ref, inner + span)):
        for c in range(0, taps.shape[1], chunk):
            series = joined[:, at + c : at + c + chunk].astype(F32)
            total = jnp.zeros((T, chunk), F32)
            for k in range(KERNEL):
                total = total + taps[k : k + 1, c : c + chunk] * series[first + k : first + k + T, :]
            conv[:, at + c : at + c + chunk] = jax.nn.silu(total).astype(BF16)

    for j in range(1, S):
        share_steps(j).wait_recv()
    for p in range(S):
        at = pl.ds(p * hc, hc)
        step_rows[at, :] = rbuf[p, pl.ds(0, hc), :]
        decay_rows[at, :] = rbuf[p, pl.ds(hc, hc), :]
        total_rows[at, :] = rbuf[p, pl.ds(2 * hc, hc), :]
    steps = step_rows[...]
    cumulative = lane_scan(decay_rows[...], T)
    final = jnp.sum(jnp.where(iota((H, T), 1) == T - 1, cumulative, 0.0), axis=1, keepdims=True)
    rows[0:H, :] = cumulative
    rows[H : 2 * H, :] = jnp.exp(final - cumulative) * steps
    rows[2 * H : 3 * H, :] = jnp.exp(cumulative)
    cols[...] = rows[...].T

    lane = iota((T, pair), 1)
    low = lane < HEAD_DIM

    def by_head(base, q):
        return jnp.where(
            low, cols[:, base + 2 * q : base + 2 * q + 1], cols[:, base + 2 * q + 1 : base + 2 * q + 2]
        )

    for q in range(H // 2):
        at = pl.ds(q * pair, pair)
        scaled[:, at] = (conv[:, at].astype(F32) * by_head(H, q)).astype(BF16)
    for p in range(G // 2):
        b_pair = conv[:, inner + p * pair : inner + (p + 1) * pair]
        both = lax.dot_general(
            b_pair, scaled[:, 2 * gw * p : 2 * gw * (p + 1)], (((0,), (0,)), ((), ())),
            preferred_element_type=F32,
        )
        for i in range(2):
            state[2 * p + i] = both[i * STATE : (i + 1) * STATE, i * gw : (i + 1) * gw]

    lanes_h = iota((H, T), 1)
    through = lane_scan(total_rows[...], S)
    ahead_of = through - total_rows[...]

    def pick(values, index):
        return jnp.sum(jnp.where(lanes_h == index, values, 0.0), axis=1, keepdims=True)

    head_of = iota((H, inner), 1) // HEAD_DIM == iota((H, inner), 0)

    def spread(column):
        return jnp.sum(jnp.where(head_of, column, 0.0), axis=0, keepdims=True)

    at_plane = pick(ahead_of, zi * Y)
    at_next = pick(ahead_of, zi * Y + Y)
    at_here = pick(ahead_of, s)
    past_here = pick(through, s)
    zf = spread(jnp.exp(at_next - at_plane))
    zs = spread(jnp.exp(at_next - past_here))
    own_f = spread(jnp.exp(at_here - at_plane))
    yf, ys = [None], [None]
    for dy in range(1, Y):
        at_peer = pick(ahead_of, flip(s, dy))
        later = flip(s, dy) > s
        yf.append(spread(jnp.exp(at_peer - at_plane)))
        ys.append(spread(jnp.where(later, jnp.exp(jnp.minimum(at_peer - past_here, 0.0)), 0.0)))

    def column(values, g):
        return values[:, g * gw : (g + 1) * gw]

    def along_z(g):
        return remote(sendz.at[g], recvz.at[g], z_s.at[g], z_r.at[g], {"sp": s + Y})

    def along_y(dy, g):
        return remote(
            sendy.at[dy - 1, g], recvy.at[dy - 1, g], y_s.at[dy - 1, g], y_r.at[dy - 1, g],
            {"sp": flip(s, dy)},
        )

    @pl.when(zi == 0)
    def _():
        for g in range(G):
            sendz[g] = (column(zs, g) * state[g]).astype(BF16)
            along_z(g).start()

    causal = iota((T, T), 0) >= iota((T, T), 1)
    for g in range(G):
        p, i = g // 2, g % 2
        at_b = inner + p * pair
        at_c = inner + span + p * pair
        half = low if i == 0 else jnp.logical_not(low)
        c_half = jnp.where(half, conv[:, at_c : at_c + pair].astype(F32), 0.0).astype(BF16)
        cmask[g] = c_half
        scores = lax.dot_general(
            c_half, conv[:, at_b : at_b + pair], (((1,), (1,)), ((), ())),
            preferred_element_type=F32,
        )
        per = H // G // 2
        for q in range(g * per, (g + 1) * per):
            at = pl.ds(q * pair, pair)
            mixes = []
            for h in (2 * q, 2 * q + 1):
                gap = jnp.where(causal, cols[:, h : h + 1] - rows[h : h + 1, :], -jnp.inf)
                mixes.append((scores * jnp.exp(gap) * step_rows[h : h + 1, :]).astype(BF16))
            x_pair = conv[:, at].astype(F32)
            stacked = jnp.concatenate(
                [jnp.where(low, x_pair, 0.0).astype(BF16), jnp.where(low, 0.0, x_pair).astype(BF16)],
                axis=0,
            )
            diag[:, at] = jnp.dot(
                jnp.concatenate(mixes, axis=1), stacked, preferred_element_type=F32
            )

    for g in range(G):
        @pl.when(zi > 0)
        def _():
            along_z(g).wait_recv()

        @pl.when(jnp.logical_and(zi > 0, zi < Z - 1))
        def _():
            sendz[g] = (column(zf, g) * recvz[g].astype(F32) + column(zs, g) * state[g]).astype(BF16)
            along_z(g).start()

        for dy in range(1, Y):
            sendy[dy - 1, g] = (
                column(yf[dy], g) * recvz[g].astype(F32) + column(ys[dy], g) * state[g]
            ).astype(BF16)
            along_y(dy, g).start()

    for load in loads[3:]:
        load.wait()
    for g in range(G):
        at = pl.ds(g * gw, gw)
        entering = column(own_f, g) * recvz[g].astype(F32)
        for dy in range(1, Y):
            along_y(dy, g).wait_recv()
            entering = entering + recvy[dy - 1, g].astype(F32)
        high = entering.astype(BF16)
        rest = (entering - high.astype(F32)).astype(BF16)
        c_half = cmask[g]
        carried = jnp.dot(
            c_half, jnp.concatenate([high, high], axis=0), preferred_element_type=F32
        ) + jnp.dot(c_half, jnp.concatenate([rest, rest], axis=0), preferred_element_type=F32)
        per = H // G // 2
        reach = jnp.concatenate([by_head(2 * H, q) for q in range(g * per, (g + 1) * per)], axis=1)
        mixed = (diag[:, at] + carried * reach).astype(BF16)
        gated = mixed.astype(F32) * jax.nn.silu(valve[:, at].astype(F32))
        power = jnp.mean(gated * gated, axis=-1, keepdims=True)
        normed_g[:, at] = (gated * lax.rsqrt(power + RMS_EPS) * gain_ref[:, at]).astype(BF16)
        base = skip[...].astype(F32) if g == 0 else pre[...]
        pre[...] = base + jnp.dot(normed_g[:, at], wo[at, :], preferred_element_type=F32)

    tile = 16

    def normalise(i, carry):
        at = pl.ds(pl.multiple_of(i * tile, tile), tile)
        value = pre[at, :]
        centre = jnp.mean(value, axis=-1, keepdims=True)
        gap = value - centre
        variance = jnp.mean(gap * gap, axis=-1, keepdims=True)
        normed[at, :] = (
            gap * lax.rsqrt(variance + NORM_EPS) * lns_ref[...] + lno_ref[...]
        ).astype(BF16)
        return carry

    lax.fori_loop(0, T // tile, normalise, 0)

    issue, plan = expert_plan(S)

    def slot_rows(j, dc, dx, count=1):
        return pl.ds((j * R + dc * nx + dx) * cap, count * cap)

    def disp(j):
        return remote(outb.at[pl.ds(j * cap, cap)], arr.at[slot_rows(j, 0, 0)],
                      d_s.at[j], d_r.at[j], {"sp": flip(s, j)})

    def agx(j, dx):
        return remote(arr.at[slot_rows(j, 0, 0)], arr.at[slot_rows(j, 0, dx)],
                      g_s.at[j, dx], g_r.at[j, dx], {"dp": flip(d, 2 * dx)})

    def agc(j, dx):
        return remote(arr.at[slot_rows(j, 0, dx)], arr.at[slot_rows(j, 1, dx)],
                      g_s.at[j, nx + dx], g_r.at[j, nx + dx], {"dp": flip(d, 1)})

    def rsc(j):
        return remote(arr.at[slot_rows(j, 1, 0, nx)], ra.at[pl.ds(j * nx * cap, nx * cap)],
                      a_s.at[j], a_r.at[j], {"dp": flip(d, 1)})

    def rsx(j, dx):
        at = pl.ds((j * (nx - 1) + dx - 1) * cap, cap)
        return remote(sx.at[at], rx.at[at], x_s.at[j, dx], x_r.at[j, dx], {"dp": flip(d, 2 * dx)})

    def back(j):
        return remote(outb.at[pl.ds(j * cap, cap)], ret.at[pl.ds(j * cap, cap)],
                      b_s.at[j], b_r.at[j], {"sp": flip(s, j)})

    def place(j):
        slot = iota((cap, T), 0) + j * cap
        hit = jnp.logical_or(slot == targets[0], slot == targets[1])
        moved = jnp.dot(
            hit.astype(F32).astype(BF16), normed[...], preferred_element_type=F32
        ).astype(BF16)
        if j:
            outb[pl.ds(j * cap, cap), :] = moved
            disp(j).start()
        else:
            arr[slot_rows(0, 0, 0), :] = moved

    for j in issue:
        place(j)

    def arrive(j):
        if j:
            disp(j).wait_recv()
        for dx in range(1, nx):
            agx(j, dx).start()
        agc(j, 0).start()

    def relay(j):
        for dx in range(1, nx):
            agx(j, dx).wait_recv()
            agc(j, dx).start()

    def gate_up(j):
        for dx in range(nx):
            agc(j, dx).wait_recv()
        wide = 256 if ff % 256 == 0 else 128

        def piece(i, carry):
            at = pl.ds(pl.multiple_of(i * wide, wide), wide)
            x = arr[slot_rows(j, 0, 0, R), :]
            g = jnp.dot(x, wg[:, at], preferred_element_type=F32)
            u = jnp.dot(x, wu[:, at], preferred_element_type=F32)
            hid[:, at] = (jax.nn.silu(g) * u).astype(BF16)
            return carry

        lax.fori_loop(0, ff // wide, piece, 0)

    def down(j):
        for dx in range(nx):
            if dx:
                agx(j, dx).wait_send()
            agc(j, dx).wait_send()
        wide = 256 if width % 256 == 0 else 128

        def piece(i, carry):
            at = pl.ds(pl.multiple_of(i * wide, wide), wide)
            arr[slot_rows(j, 0, 0, R), at] = jnp.dot(
                hid[...], wd[:, at], preferred_element_type=F32
            ).astype(BF16)
            return carry

        lax.fori_loop(0, width // wide, piece, 0)
        rsc(j).start()

    def chip_sum(j):
        rsc(j).wait_recv()
        for dx in range(1, nx):
            both = (
                arr[slot_rows(j, 0, dx), :].astype(F32)
                + ra[pl.ds((j * nx + dx) * cap, cap), :].astype(F32)
            )
            sx[pl.ds((j * (nx - 1) + dx - 1) * cap, cap), :] = both.astype(BF16)
            rsx(j, dx).start()

    def finish(j):
        total = (
            arr[slot_rows(j, 0, 0), :].astype(F32)
            + ra[pl.ds(j * nx * cap, cap), :].astype(F32)
        )
        for dx in range(1, nx):
            rsx(j, dx).wait_recv()
            total = total + rx[pl.ds((j * (nx - 1) + dx - 1) * cap, cap), :].astype(F32)
        if j:
            disp(j).wait_send()
            outb[pl.ds(j * cap, cap), :] = total.astype(BF16)
            back(j).start()
        else:
            ret[pl.ds(0, cap), :] = total.astype(BF16)

    stages = dict(A=arrive, R=relay, G=gate_up, D=down, C=chip_sum, F=finish)
    for at, (stage, j) in enumerate(plan):
        if stage == "G" and not any(name == "G" for name, _ in plan[:at]):
            weights[0].wait()
            weights[1].wait()
        if stage == "D" and not any(name == "D" for name, _ in plan[:at]):
            weights[2].wait()
        stages[stage](j)

    target_cols = [cols[:, 3 * H + k : 3 * H + k + 1].astype(I32) for k in range(2)]
    shares = [cols[:, 3 * H + 2 + k : 3 * H + 3 + k] for k in range(2)]
    pre[...] = normed[...].astype(F32)
    for j in [0] + [j for stage, j in plan if stage == "F" and j]:
        if j:
            back(j).wait_recv()
        slot = iota((T, cap), 1) + j * cap
        hit = jnp.logical_or(slot == target_cols[0], slot == target_cols[1])
        share = jnp.zeros((T, 1), F32)
        for k in range(2):
            inside = jnp.logical_and(target_cols[k] >= j * cap, target_cols[k] < (j + 1) * cap)
            share = share + jnp.where(inside, shares[k], 0.0)
        moved = jnp.dot(
            hit.astype(F32).astype(BF16), ret[pl.ds(j * cap, cap), :], preferred_element_type=F32
        )
        pre[...] = pre[...] + share * moved
    out_ref[...] = pre[...].astype(BF16)

    for j in range(1, S):
        share_steps(j).wait_send()

    @pl.when(s < S - 1)
    def _():
        halo_to().wait_send()

    @pl.when(zi < Z - 1)
    def _():
        for g in range(G):
            along_z(g).wait_send()

    for g in range(G):
        for dy in range(1, Y):
            along_y(dy, g).wait_send()
    for j in range(S):
        rsc(j).wait_send()
        for dx in range(1, nx):
            rsx(j, dx).wait_send()
        if j:
            back(j).wait_send()


def run_layer(S, R, cap, big, small):
    xs, bs, cs, valve, skip, wo, wg, wu, wd = big
    T, inner = xs.shape
    span = bs.shape[1]
    width = skip.shape[1]
    ff = wg.shape[1]
    nx = R // 2
    Y = 1
    while Y * Y * 4 <= S:
        Y *= 2
    gw = inner // GROUPS
    dma = pltpu.SemaphoreType.DMA
    vmem = pltpu.VMEM
    total = S * R * cap
    whole = inner + 2 * span
    buffers = [
        vmem((HALO + T, whole), BF16),
        vmem((T, whole), BF16),
        vmem((T, inner), BF16),
        vmem((T, width), BF16),
        vmem((inner, width), BF16),
        vmem((S, 8, T), F32),
        vmem((S, 8, T), F32),
        vmem((HEADS, T), F32),
        vmem((HEADS, T), F32),
        vmem((HEADS, T), F32),
        vmem((T, T), F32),
        vmem((T, T), F32),
        vmem((GROUPS, T, 2 * STATE), BF16),
        vmem((T, inner), F32),
        vmem((T, inner), BF16),
        vmem((GROUPS, STATE, gw), F32),
        vmem((GROUPS, STATE, gw), BF16),
        vmem((GROUPS, STATE, gw), BF16),
        vmem((Y - 1, GROUPS, STATE, gw), BF16),
        vmem((Y - 1, GROUPS, STATE, gw), BF16),
        vmem((T, inner), BF16),
        vmem((T, width), F32),
        vmem((T, width), BF16),
        vmem((S * cap, width), BF16),
        vmem((total, width), BF16),
        vmem((R * cap, ff), BF16),
        vmem((S * nx * cap, width), BF16),
        vmem((S * (nx - 1) * cap, width), BF16),
        vmem((S * (nx - 1) * cap, width), BF16),
        vmem((S * cap, width), BF16),
        vmem((width, ff), BF16),
        vmem((width, ff), BF16),
        vmem((ff, width), BF16),
    ]
    held = sum(b.dtype.itemsize * math.prod(b.shape) for b in buffers)
    limit = min(62 * 2**20, held + 12 * 2**20)
    return pl.pallas_call(
        functools.partial(layer_kernel, S, R, Y, cap),
        out_shape=jax.ShapeDtypeStruct((T, width), BF16),
        in_specs=[pl.BlockSpec(memory_space=pl.ANY)] * 9
        + [pl.BlockSpec(memory_space=pltpu.VMEM)] * 2
        + [pl.BlockSpec(memory_space=pltpu.SMEM)]
        + [pl.BlockSpec(memory_space=pltpu.VMEM)] * 8,
        out_specs=pl.BlockSpec(memory_space=pltpu.VMEM),
        scratch_shapes=buffers + [
            dma((6,)), dma((3,)),
            dma((S,)), dma((S,)),
            dma(()), dma(()),
            dma((GROUPS,)), dma((GROUPS,)),
            dma((Y - 1, GROUPS)), dma((Y - 1, GROUPS)),
            dma((S,)), dma((S,)),
            dma((S, R)), dma((S, R)),
            dma((S,)), dma((S,)),
            dma((S, nx)), dma((S, nx)),
            dma((S,)), dma((S,)),
        ],
        compiler_params=pltpu.CompilerParams(
            collective_id=0, has_side_effects=True, vmem_limit_bytes=limit
        ),
        cost_estimate=pl.CostEstimate(
            flops=6 * total * width * ff, bytes_accessed=6 * width * ff, transcendentals=total * ff
        ),
    )(*big, *small)


def per_device(
    skip_connection_stream,
    emitted_valve_unscaled,
    channel_source_mapped,
    hidden_source_mapped,
    probe_mapped_values,
    increment_premapped,
    extra_log_fading,
    channel_fading_speed,
    channel_source_kernel,
    hidden_source_kernel,
    probe_kernel_coefficients,
    cluster_scaling_factor,
    emitted_mapping_matrix,
    standardize_scaling,
    standardize_offset,
    chosen_specialist_ids,
    specialist_mixing_shares,
    specialist_gating_matrices,
    raising_matrices,
    lowering_matrices,
):
    S = lax.axis_size("sp")
    R = lax.axis_size("dp")
    T = skip_connection_stream.shape[1]
    assert T == BLK
    cap = -(-(3 * T // S) // 16) * 16
    big = (
        channel_source_mapped[0], hidden_source_mapped[0], probe_mapped_values[0],
        emitted_valve_unscaled[0], skip_connection_stream[0], emitted_mapping_matrix,
        specialist_gating_matrices[0], raising_matrices[0], lowering_matrices[0],
    )
    small = (
        increment_premapped[0].T, extra_log_fading[0].T, channel_fading_speed,
        channel_source_kernel, hidden_source_kernel, probe_kernel_coefficients,
        cluster_scaling_factor[None, :], standardize_scaling[None, :], standardize_offset[None, :],
        chosen_specialist_ids[0].T, specialist_mixing_shares[0].T,
    )
    return run_layer(S, R, cap, big, small)[None]


def solution(mesh):
    placed = (
        P("dp", "sp", None),
        P("dp", "sp", None),
        P("dp", "sp", None),
        P("dp", "sp", None),
        P("dp", "sp", None),
        P("dp", None, "sp"),
        P("dp", None, "sp"),
        P(),
        P(),
        P(),
        P(),
        P(),
        P(),
        P(),
        P(),
        P("dp", "sp", None),
        P("dp", "sp", None),
        P("sp", None, "dp"),
        P("sp", None, "dp"),
        P("sp", "dp", None),
    )
    return jax.shard_map(
        per_device, mesh=mesh, in_specs=placed, out_specs=P("dp", "sp", None), check_vma=False
    )
```

```python
import functools

import jax
import jax.numpy as jnp
from jax import lax
from jax.experimental import pallas as pl
from jax.experimental.pallas import tpu as pltpu
from jax.sharding import PartitionSpec as P

HEADS = 16
HEAD_DIM = 64
GROUPS = 4
STATE = 64
KERNEL = 4
BLK = 128

RMS_EPS = 1e-06
NORM_EPS = 1e-05
HALO = 16
PARTS = 1
MESH = pl.DeviceIdType.MESH
F32 = jnp.float32
BF16 = jnp.bfloat16
I32 = jnp.int32


def flip(value, mask):
    result, bit = value, 1
    while bit <= mask:
        if mask & bit:
            result = result + bit * (1 - 2 * ((value // bit) % 2))
        bit *= 2
    return result


def iota(shape, dim):
    return lax.broadcasted_iota(I32, shape, dim)


def lane_scan(value, width):
    lanes = iota(value.shape, 1)
    step = 1
    while step < width:
        value = value + jnp.where(lanes >= step, pltpu.roll(value, step, 1), 0.0)
        step *= 2
    return value


ISSUE_OF_8 = (
    50, 60, 20, 30, 70, 40, 10,
)
PLAN_OF_8 = (
    0, 50, 10, 150, 60, 250, 350, 20, 160, 450, 260, 70, 30, 120, 360, 100, 220, 320, 170, 420, 270, 550, 130,
    460, 110, 370, 230, 40, 470, 520, 330, 560, 210, 430, 140, 310, 240, 570, 340, 440, 530, 410, 200, 300,
    540, 400, 510, 500,
)


def expert_plan(S):
    if S == 8:
        return (
            [(0, h) for h in range(PARTS)] + [divmod(code, 10) for code in ISSUE_OF_8],
            [(code // 100, code // 10 % 10, code % 10) for code in PLAN_OF_8],
        )
    order = list(range(S))
    plan = [(0, j) for j in order[:2]]
    for p, j in enumerate(order):
        plan += [(1, j), (2, j)]
        if p + 2 < S:
            plan.append((0, order[p + 2]))
        if p > 1:
            plan.append((5, order[p - 2]))
        if p:
            plan.append((4, order[p - 1]))
        plan.append((3, j))
    if S > 1:
        plan.append((5, order[S - 2]))
    plan += [(4, order[S - 1]), (5, order[S - 1])]
    return (
        [(j, h) for j in order for h in range(PARTS)],
        [(stage, j, h) for stage, j in plan for h in range(1 if stage == 2 else PARTS)],
    )


def layer_kernel(
    S, R, Y, cap,
    xs_hbm, bs_hbm, cs_hbm, valve_hbm, skip_hbm, wo_hbm, wg_hbm, wu_hbm, wd_hbm,
    *rest,
):
    small_hbm, (out_ref, *rest) = rest[:11], rest[11:]
    small_vmem, rest = rest[:11], rest[11:]
    (
        inc_ref, fade_ref, speed_ref, xk_ref, bk_ref, ck_ref, gain_ref, lns_ref, lno_ref,
        ids_ref, share_ref,
    ) = small_vmem
    (
        joined, conv, valve, skip, wo, msg, rbuf, step_rows, decay_rows, total_rows, rows, cols,
        cmask, diag, scaled, state, sendz, recvz, sendy, recvy, normed_g, pre, normed,
        outb, arr, hid, ra, rx, sx, ret, wg, wu, wd,
        in_sem, t_sem, w_sem, m_s, m_r, h_s, h_r, z_s, z_r, y_s, y_r,
        d_s, d_r, g_s, g_r, a_s, a_r, x_s, x_r, b_s, b_r,
    ) = rest
    s = lax.axis_index("sp")
    d = lax.axis_index("dp")
    T, inner = xs_hbm.shape
    span = bs_hbm.shape[1]
    width = skip_hbm.shape[1]
    ff = wg_hbm.shape[1]
    hc = small_hbm[0].shape[0]
    H = HEADS
    G = GROUPS
    gw = inner // G
    pair = 2 * HEAD_DIM
    zi = s // Y
    yi = s % Y
    Z = S // Y
    nx = R // 2

    def remote(src, dst, send, recv, where):
        return pltpu.make_async_remote_copy(
            src_ref=src, dst_ref=dst, send_sem=send, recv_sem=recv,
            device_id=where, device_id_type=MESH,
        )

    def local(src, dst, sem):
        return pltpu.make_async_copy(src, dst, sem)

    body = pl.ds(HALO, T)
    loads = [
        local(xs_hbm, joined.at[body, pl.ds(0, inner)], in_sem.at[0]),
        local(bs_hbm, joined.at[body, pl.ds(inner, span)], in_sem.at[1]),
        local(cs_hbm, joined.at[body, pl.ds(inner + span, span)], in_sem.at[2]),
        local(valve_hbm, valve, in_sem.at[3]),
        local(skip_hbm, skip, in_sem.at[4]),
        local(wo_hbm, wo, in_sem.at[5]),
    ]
    weights = [
        local(src, dst, w_sem.at[i])
        for i, (src, dst) in enumerate(((wg_hbm, wg), (wu_hbm, wu), (wd_hbm, wd)))
    ]
    tables = [local(src, dst, t_sem.at[i]) for i, (src, dst) in enumerate(zip(small_hbm, small_vmem))]
    for load in tables[:3] + loads[:3] + tables[3:] + loads[3:]:
        load.start()

    barrier = pltpu.get_barrier_semaphore()
    peers = [{"sp": flip(s, j)} for j in range(1, S)]
    peers += [{"dp": flip(d, 1)}] + [{"dp": flip(d, 2 * dx)} for dx in range(1, nx)]
    for peer in peers:
        pl.semaphore_signal(barrier, inc=1, device_id=peer, device_id_type=MESH)

    for load in tables[:3]:
        load.wait()
    step_in = jax.nn.softplus(inc_ref[...])
    own_rows = iota((hc, 1), 0)
    speeds = jnp.zeros((hc, 1), F32)
    for i in range(hc):
        own = iota((1, H), 1) == s * hc + i
        speed = jnp.sum(jnp.where(own, speed_ref[...], 0.0), axis=1, keepdims=True)
        speeds = jnp.where(own_rows == i, speed, speeds)
    decay_in = fade_ref[...] - speeds * step_in
    tot_lanes = iota((hc, T), 1)
    totals_in = jnp.zeros((hc, T), F32)
    for j in range(S):
        block = decay_in[:, j * T : (j + 1) * T]
        totals_in = jnp.where(tot_lanes == j, jnp.sum(block, axis=1, keepdims=True), totals_in)
    for j in range(S):
        msg[j, pl.ds(0, hc), :] = step_in[:, j * T : (j + 1) * T]
        msg[j, pl.ds(hc, hc), :] = decay_in[:, j * T : (j + 1) * T]
        msg[j, pl.ds(2 * hc, hc), :] = totals_in
        msg[j, pl.ds(3 * hc, 8 - 3 * hc), :] = jnp.zeros((8 - 3 * hc, T), F32)

    pl.semaphore_wait(barrier, len(peers))

    def share_steps(j):
        return remote(msg.at[flip(s, j)], rbuf.at[s], m_s.at[j], m_r.at[j], {"sp": flip(s, j)})

    def halo_to():
        return remote(
            joined.at[pl.ds(T, HALO)], joined.at[pl.ds(0, HALO)], h_s, h_r, {"sp": s + 1}
        )

    for j in range(S - 1, 0, -1):
        share_steps(j).start()
    rbuf[s] = msg[s]

    for load in loads[:3]:
        load.wait()

    @pl.when(s < S - 1)
    def _():
        halo_to().start()

    for load in weights:
        load.start()

    @pl.when(s == 0)
    def _():
        joined[pl.ds(0, HALO), :] = jnp.zeros((HALO, joined.shape[1]), BF16)

    @pl.when(zi == 0)
    def _():
        recvz[...] = jnp.zeros(recvz.shape, BF16)

    for load in tables[3:]:
        load.wait()

    experts = iota((S, T), 0)
    hot = [(ids_ref[k : k + 1, :] == experts) for k in range(2)]
    named = (hot[0].astype(F32) + hot[1].astype(F32)).astype(BF16)
    before_t = (iota((T, T), 0) < iota((T, T), 1)).astype(F32).astype(BF16)
    ranks = jnp.dot(named, before_t, preferred_element_type=F32)
    targets = []
    for k in range(2):
        rank = jnp.sum(jnp.where(hot[k], ranks, 0.0), axis=0, keepdims=True)
        relative = jnp.bitwise_xor(ids_ref[k : k + 1, :], s)
        targets.append(relative * cap + rank.astype(I32))
        rows[3 * H + k : 3 * H + k + 1, :] = targets[k].astype(F32)
    rows[3 * H + 2 : 3 * H + 4, :] = share_ref[...]
    rows[3 * H + 4 :, :] = jnp.zeros((rows.shape[0] - 3 * H - 4, T), F32)

    @pl.when(s > 0)
    def _():
        halo_to().wait_recv()

    chunk = 256
    first = HALO - KERNEL + 1
    for taps, at in ((xk_ref, 0), (bk_ref, inner), (ck_ref, inner + span)):
        for c in range(0, taps.shape[1], chunk):
            series = joined[:, at + c : at + c + chunk].astype(F32)
            total = jnp.zeros((T, chunk), F32)
            for k in range(KERNEL):
                total = total + taps[k : k + 1, c : c + chunk] * series[first + k : first + k + T, :]
            conv[:, at + c : at + c + chunk] = jax.nn.silu(total).astype(BF16)

    for j in range(1, S):
        share_steps(j).wait_recv()
    for p in range(S):
        at = pl.ds(p * hc, hc)
        step_rows[at, :] = rbuf[p, pl.ds(0, hc), :]
        decay_rows[at, :] = rbuf[p, pl.ds(hc, hc), :]
        total_rows[at, :] = rbuf[p, pl.ds(2 * hc, hc), :]
    steps = step_rows[...]
    cumulative = lane_scan(decay_rows[...], T)
    final = jnp.sum(jnp.where(iota((H, T), 1) == T - 1, cumulative, 0.0), axis=1, keepdims=True)
    rows[0:H, :] = cumulative
    rows[H : 2 * H, :] = jnp.exp(final - cumulative) * steps
    rows[2 * H : 3 * H, :] = jnp.exp(cumulative)
    cols[...] = rows[...].T

    lane = iota((T, pair), 1)
    low = lane < HEAD_DIM

    def by_head(base, q):
        return jnp.where(
            low, cols[:, base + 2 * q : base + 2 * q + 1], cols[:, base + 2 * q + 1 : base + 2 * q + 2]
        )

    for q in range(H // 2):
        at = pl.ds(q * pair, pair)
        scaled[:, at] = (conv[:, at].astype(F32) * by_head(H, q)).astype(BF16)
    for p in range(G // 2):
        b_pair = conv[:, inner + p * pair : inner + (p + 1) * pair]
        both = lax.dot_general(
            b_pair, scaled[:, 2 * gw * p : 2 * gw * (p + 1)], (((0,), (0,)), ((), ())),
            preferred_element_type=F32,
        )
        for i in range(2):
            state[2 * p + i] = both[i * STATE : (i + 1) * STATE, i * gw : (i + 1) * gw]

    lanes_h = iota((H, T), 1)
    through = lane_scan(total_rows[...], S)
    ahead_of = through - total_rows[...]

    def pick(values, index):
        return jnp.sum(jnp.where(lanes_h == index, values, 0.0), axis=1, keepdims=True)

    head_of = iota((H, inner), 1) // HEAD_DIM == iota((H, inner), 0)

    def spread(column):
        return jnp.sum(jnp.where(head_of, column, 0.0), axis=0, keepdims=True)

    at_plane = pick(ahead_of, zi * Y)
    at_next = pick(ahead_of, zi * Y + Y)
    at_here = pick(ahead_of, s)
    past_here = pick(through, s)
    zf = spread(jnp.exp(at_next - at_plane))
    zs = spread(jnp.exp(at_next - past_here))
    own_f = spread(jnp.exp(at_here - at_plane))
    yf, ys = [None], [None]
    for dy in range(1, Y):
        at_peer = pick(ahead_of, flip(s, dy))
        later = flip(s, dy) > s
        yf.append(spread(jnp.exp(at_peer - at_plane)))
        ys.append(spread(jnp.where(later, jnp.exp(jnp.minimum(at_peer - past_here, 0.0)), 0.0)))

    def column(values, g):
        return values[:, g * gw : (g + 1) * gw]

    def along_z(g):
        return remote(sendz.at[g], recvz.at[g], z_s.at[g], z_r.at[g], {"sp": s + Y})

    def along_y(dy, g):
        return remote(
            sendy.at[dy - 1, g], recvy.at[dy - 1, g], y_s.at[dy - 1, g], y_r.at[dy - 1, g],
            {"sp": flip(s, dy)},
        )

    @pl.when(zi == 0)
    def _():
        for g in range(G):
            sendz[g] = (column(zs, g) * state[g]).astype(BF16)
            along_z(g).start()

    causal = iota((T, T), 0) >= iota((T, T), 1)
    for g in range(G):
        p, i = g // 2, g % 2
        at_b = inner + p * pair
        at_c = inner + span + p * pair
        half = low if i == 0 else jnp.logical_not(low)
        c_half = jnp.where(half, conv[:, at_c : at_c + pair].astype(F32), 0.0).astype(BF16)
        cmask[g] = c_half
        scores = lax.dot_general(
            c_half, conv[:, at_b : at_b + pair], (((1,), (1,)), ((), ())),
            preferred_element_type=F32,
        )
        per = H // G // 2
        for q in range(g * per, (g + 1) * per):
            at = pl.ds(q * pair, pair)
            mixes = []
            for h in (2 * q, 2 * q + 1):
                gap = jnp.where(causal, cols[:, h : h + 1] - rows[h : h + 1, :], -jnp.inf)
                mixes.append((scores * jnp.exp(gap) * step_rows[h : h + 1, :]).astype(BF16))
            x_pair = conv[:, at].astype(F32)
            stacked = jnp.concatenate(
                [jnp.where(low, x_pair, 0.0).astype(BF16), jnp.where(low, 0.0, x_pair).astype(BF16)],
                axis=0,
            )
            diag[:, at] = jnp.dot(
                jnp.concatenate(mixes, axis=1), stacked, preferred_element_type=F32
            )

    for g in range(G):
        @pl.when(zi > 0)
        def _():
            along_z(g).wait_recv()

        @pl.when(jnp.logical_and(zi > 0, zi < Z - 1))
        def _():
            sendz[g] = (column(zf, g) * recvz[g].astype(F32) + column(zs, g) * state[g]).astype(BF16)
            along_z(g).start()

        for dy in range(1, Y):
            sendy[dy - 1, g] = (
                column(yf[dy], g) * recvz[g].astype(F32) + column(ys[dy], g) * state[g]
            ).astype(BF16)
            along_y(dy, g).start()

    for load in loads[3:]:
        load.wait()
    for g in range(G):
        at = pl.ds(g * gw, gw)
        entering = column(own_f, g) * recvz[g].astype(F32)
        for dy in range(1, Y):
            along_y(dy, g).wait_recv()
            entering = entering + recvy[dy - 1, g].astype(F32)
        high = entering.astype(BF16)
        rest = (entering - high.astype(F32)).astype(BF16)
        c_half = cmask[g]
        carried = jnp.dot(
            c_half, jnp.concatenate([high, high], axis=0), preferred_element_type=F32
        ) + jnp.dot(c_half, jnp.concatenate([rest, rest], axis=0), preferred_element_type=F32)
        per = H // G // 2
        reach = jnp.concatenate([by_head(2 * H, q) for q in range(g * per, (g + 1) * per)], axis=1)
        mixed = (diag[:, at] + carried * reach).astype(BF16)
        gated = mixed.astype(F32) * jax.nn.silu(valve[:, at].astype(F32))
        power = jnp.mean(gated * gated, axis=-1, keepdims=True)
        normed_g[:, at] = (gated * lax.rsqrt(power + RMS_EPS) * gain_ref[:, at]).astype(BF16)
        base = skip[...].astype(F32) if g == 0 else pre[...]
        pre[...] = base + jnp.dot(normed_g[:, at], wo[at, :], preferred_element_type=F32)

    tile = 16

    def normalise(i, carry):
        at = pl.ds(pl.multiple_of(i * tile, tile), tile)
        value = pre[at, :]
        centre = jnp.mean(value, axis=-1, keepdims=True)
        gap = value - centre
        variance = jnp.mean(gap * gap, axis=-1, keepdims=True)
        normed[at, :] = (
            gap * lax.rsqrt(variance + NORM_EPS) * lns_ref[...] + lno_ref[...]
        ).astype(BF16)
        return carry

    lax.fori_loop(0, T // tile, normalise, 0)

    issue, plan = expert_plan(S)

    half_width = width // PARTS

    def half(h):
        return pl.ds(h * half_width, half_width)

    def slot_rows(j, dc, dx, count=1):
        return pl.ds((j * R + dc * nx + dx) * cap, count * cap)

    def of(j):
        return pl.ds(j * cap, cap)

    def beside(j, dx):
        return pl.ds((j * (nx - 1) + dx - 1) * cap, cap)

    def disp(j, h):
        return remote(outb.at[of(j), half(h)], arr.at[slot_rows(j, 0, 0), half(h)],
                      d_s.at[j, h], d_r.at[j, h], {"sp": flip(s, j)})

    def agx(j, dx, h):
        return remote(arr.at[slot_rows(j, 0, 0), half(h)], arr.at[slot_rows(j, 0, dx), half(h)],
                      g_s.at[j, dx, h], g_r.at[j, dx, h], {"dp": flip(d, 2 * dx)})

    def agc(j, dx, h):
        return remote(arr.at[slot_rows(j, 0, dx), half(h)], arr.at[slot_rows(j, 1, dx), half(h)],
                      g_s.at[j, nx + dx, h], g_r.at[j, nx + dx, h], {"dp": flip(d, 1)})

    def rsc(j, h):
        return remote(arr.at[slot_rows(j, 1, 0, nx), half(h)],
                      ra.at[pl.ds(j * nx * cap, nx * cap), half(h)],
                      a_s.at[j, h], a_r.at[j, h], {"dp": flip(d, 1)})

    def rsx(j, dx, h):
        return remote(sx.at[beside(j, dx), half(h)], rx.at[beside(j, dx), half(h)],
                      x_s.at[j, dx, h], x_r.at[j, dx, h], {"dp": flip(d, 2 * dx)})

    def back(j, h):
        return remote(outb.at[of(j), half(h)], ret.at[of(j), half(h)],
                      b_s.at[j, h], b_r.at[j, h], {"sp": flip(s, j)})

    def place(j, h):
        slot = iota((cap, T), 0) + j * cap
        hit = jnp.logical_or(slot == targets[0], slot == targets[1])
        moved = jnp.dot(
            hit.astype(F32).astype(BF16), normed[:, half(h)], preferred_element_type=F32
        ).astype(BF16)
        if j:
            outb[of(j), half(h)] = moved
            disp(j, h).start()
        else:
            arr[slot_rows(0, 0, 0), half(h)] = moved

    for j, h in issue:
        place(j, h)

    def arrive(j, h):
        if j:
            disp(j, h).wait_recv()
        for dx in range(1, nx):
            agx(j, dx, h).start()
        agc(j, 0, h).start()

    def relay(j, h):
        for dx in range(1, nx):
            agx(j, dx, h).wait_recv()
            agc(j, dx, h).start()

    def gate_up(j, _):
        for h in range(PARTS):
            for dx in range(nx):
                agc(j, dx, h).wait_recv()
        wide = 256 if ff % 256 == 0 else 128

        def piece(i, carry):
            at = pl.ds(pl.multiple_of(i * wide, wide), wide)
            x = arr[slot_rows(j, 0, 0, R), :]
            g = jnp.dot(x, wg[:, at], preferred_element_type=F32)
            u = jnp.dot(x, wu[:, at], preferred_element_type=F32)
            hid[:, at] = (jax.nn.silu(g) * u).astype(BF16)
            return carry

        lax.fori_loop(0, ff // wide, piece, 0)

    def down(j, h):
        for dx in range(nx):
            if dx:
                agx(j, dx, h).wait_send()
            agc(j, dx, h).wait_send()
        wide = 256 if half_width % 256 == 0 else 128

        def piece(i, carry):
            at = pl.ds(pl.multiple_of(h * half_width + i * wide, wide), wide)
            arr[slot_rows(j, 0, 0, R), at] = jnp.dot(
                hid[...], wd[:, at], preferred_element_type=F32
            ).astype(BF16)
            return carry

        lax.fori_loop(0, half_width // wide, piece, 0)
        rsc(j, h).start()

    def chip_sum(j, h):
        rsc(j, h).wait_recv()
        for dx in range(1, nx):
            both = (
                arr[slot_rows(j, 0, dx), half(h)].astype(F32)
                + ra[pl.ds((j * nx + dx) * cap, cap), half(h)].astype(F32)
            )
            sx[beside(j, dx), half(h)] = both.astype(BF16)
            rsx(j, dx, h).start()

    def finish(j, h):
        total = (
            arr[slot_rows(j, 0, 0), half(h)].astype(F32)
            + ra[pl.ds(j * nx * cap, cap), half(h)].astype(F32)
        )
        for dx in range(1, nx):
            rsx(j, dx, h).wait_recv()
            total = total + rx[beside(j, dx), half(h)].astype(F32)
        if j:
            disp(j, h).wait_send()
            outb[of(j), half(h)] = total.astype(BF16)
            back(j, h).start()
        else:
            ret[of(0), half(h)] = total.astype(BF16)

    stages = (arrive, relay, gate_up, down, chip_sum, finish)
    seen = set()
    for stage, j, h in plan:
        if stage == 2 and stage not in seen:
            weights[0].wait()
            weights[1].wait()
        if stage == 3 and stage not in seen:
            weights[2].wait()
        seen.add(stage)
        stages[stage](j, h)

    target_cols = [cols[:, 3 * H + k : 3 * H + k + 1].astype(I32) for k in range(2)]
    shares = [cols[:, 3 * H + 2 + k : 3 * H + 3 + k] for k in range(2)]
    pre[...] = normed[...].astype(F32)
    ends = [(j, h) for stage, j, h in plan if stage == 5]
    for j, h in [end for end in ends if end[0] == 0] + [end for end in ends if end[0]]:
        if j:
            back(j, h).wait_recv()
        slot = iota((T, cap), 1) + j * cap
        hit = jnp.logical_or(slot == target_cols[0], slot == target_cols[1])
        share = jnp.zeros((T, 1), F32)
        for k in range(2):
            inside = jnp.logical_and(target_cols[k] >= j * cap, target_cols[k] < (j + 1) * cap)
            share = share + jnp.where(inside, shares[k], 0.0)
        moved = jnp.dot(
            hit.astype(F32).astype(BF16), ret[of(j), half(h)], preferred_element_type=F32
        )
        pre[:, half(h)] = pre[:, half(h)] + share * moved
    out_ref[...] = pre[...].astype(BF16)

    for j in range(1, S):
        share_steps(j).wait_send()

    @pl.when(s < S - 1)
    def _():
        halo_to().wait_send()

    @pl.when(zi < Z - 1)
    def _():
        for g in range(G):
            along_z(g).wait_send()

    for g in range(G):
        for dy in range(1, Y):
            along_y(dy, g).wait_send()
    for h in range(PARTS):
        for j in range(S):
            rsc(j, h).wait_send()
            for dx in range(1, nx):
                rsx(j, dx, h).wait_send()
            if j:
                back(j, h).wait_send()


def run_layer(S, R, cap, big, small):
    xs, bs, cs, valve, skip, wo, wg, wu, wd = big
    T, inner = xs.shape
    span = bs.shape[1]
    width = skip.shape[1]
    ff = wg.shape[1]
    nx = R // 2
    Y = 1
    while Y * Y * 4 <= S:
        Y *= 2
    gw = inner // GROUPS
    dma = pltpu.SemaphoreType.DMA
    vmem = pltpu.VMEM
    total = S * R * cap
    whole = inner + 2 * span
    buffers = [vmem(table.shape, table.dtype) for table in small] + [
        vmem((HALO + T, whole), BF16),
        vmem((T, whole), BF16),
        vmem((T, inner), BF16),
        vmem((T, width), BF16),
        vmem((inner, width), BF16),
        vmem((S, 8, T), F32),
        vmem((S, 8, T), F32),
        vmem((HEADS, T), F32),
        vmem((HEADS, T), F32),
        vmem((HEADS, T), F32),
        vmem((T, T), F32),
        vmem((T, T), F32),
        vmem((GROUPS, T, 2 * STATE), BF16),
        vmem((T, inner), F32),
        vmem((T, inner), BF16),
        vmem((GROUPS, STATE, gw), F32),
        vmem((GROUPS, STATE, gw), BF16),
        vmem((GROUPS, STATE, gw), BF16),
        vmem((Y - 1, GROUPS, STATE, gw), BF16),
        vmem((Y - 1, GROUPS, STATE, gw), BF16),
        vmem((T, inner), BF16),
        vmem((T, width), F32),
        vmem((T, width), BF16),
        vmem((S * cap, width), BF16),
        vmem((total, width), BF16),
        vmem((R * cap, ff), BF16),
        vmem((S * nx * cap, width), BF16),
        vmem((S * (nx - 1) * cap, width), BF16),
        vmem((S * (nx - 1) * cap, width), BF16),
        vmem((S * cap, width), BF16),
        vmem((width, ff), BF16),
        vmem((width, ff), BF16),
        vmem((ff, width), BF16),
    ]
    return pl.pallas_call(
        functools.partial(layer_kernel, S, R, Y, cap),
        out_shape=jax.ShapeDtypeStruct((T, width), BF16),
        in_specs=[pl.BlockSpec(memory_space=pl.ANY)] * 20,
        out_specs=pl.BlockSpec(memory_space=pltpu.VMEM),
        scratch_shapes=buffers + [
            dma((6,)), dma((11,)), dma((3,)),
            dma((S,)), dma((S,)),
            dma(()), dma(()),
            dma((GROUPS,)), dma((GROUPS,)),
            dma((Y - 1, GROUPS)), dma((Y - 1, GROUPS)),
            dma((S, PARTS)), dma((S, PARTS)),
            dma((S, R, PARTS)), dma((S, R, PARTS)),
            dma((S, PARTS)), dma((S, PARTS)),
            dma((S, nx, PARTS)), dma((S, nx, PARTS)),
            dma((S, PARTS)), dma((S, PARTS)),
        ],
        compiler_params=pltpu.CompilerParams(
            collective_id=0, has_side_effects=True, vmem_limit_bytes=62 * 2**20
        ),
        cost_estimate=pl.CostEstimate(
            flops=6 * total * width * ff, bytes_accessed=6 * width * ff, transcendentals=total * ff
        ),
    )(*big, *small)


def per_device(
    skip_connection_stream,
    emitted_valve_unscaled,
    channel_source_mapped,
    hidden_source_mapped,
    probe_mapped_values,
    increment_premapped,
    extra_log_fading,
    channel_fading_speed,
    channel_source_kernel,
    hidden_source_kernel,
    probe_kernel_coefficients,
    cluster_scaling_factor,
    emitted_mapping_matrix,
    standardize_scaling,
    standardize_offset,
    chosen_specialist_ids,
    specialist_mixing_shares,
    specialist_gating_matrices,
    raising_matrices,
    lowering_matrices,
):
    S = lax.axis_size("sp")
    R = lax.axis_size("dp")
    T = skip_connection_stream.shape[1]
    assert T == BLK
    cap = -(-(3 * T // S) // 16) * 16
    big = (
        channel_source_mapped[0], hidden_source_mapped[0], probe_mapped_values[0],
        emitted_valve_unscaled[0], skip_connection_stream[0], emitted_mapping_matrix,
        specialist_gating_matrices[0], raising_matrices[0], lowering_matrices[0],
    )
    small = (
        increment_premapped[0].T, extra_log_fading[0].T, channel_fading_speed[None, :],
        channel_source_kernel, hidden_source_kernel, probe_kernel_coefficients,
        cluster_scaling_factor[None, :], standardize_scaling[None, :], standardize_offset[None, :],
        chosen_specialist_ids[0].T, specialist_mixing_shares[0].T,
    )
    return run_layer(S, R, cap, big, small)[None]


def solution(mesh):
    placed = (
        P("dp", "sp", None),
        P("dp", "sp", None),
        P("dp", "sp", None),
        P("dp", "sp", None),
        P("dp", "sp", None),
        P("dp", None, "sp"),
        P("dp", None, "sp"),
        P(),
        P(),
        P(),
        P(),
        P(),
        P(),
        P(),
        P(),
        P("dp", "sp", None),
        P("dp", "sp", None),
        P("sp", None, "dp"),
        P("sp", None, "dp"),
        P("sp", "dp", None),
    )
    return jax.shard_map(
        per_device, mesh=mesh, in_specs=placed, out_specs=P("dp", "sp", None), check_vma=False
    )
```
